32 devices in a mesh: sp: 8 (over z, core), tp: 4 (over y, x).
Axes of the slice: x: 2, y: 2, z: 4, core: 2. Of those that a mesh axis runs over, the one named last changes fastest.
Arguments:
- routes: int32 [1536, 2], P('sp'), may hold values from 0 to 7, all different within a row; in each aligned block of 192 rows (0 to 191, 192 to 383, ...) at most 72 rows name the same one
- route_weights: float32 [1536, 2], P('sp'), may hold values from 0.2 to 1
- expert_inputs: bfloat16 [1536, 2048], P('sp', 'tp'), may hold values from -6 to 6
- out_grad: bfloat16 [1536, 2048], P('sp', 'tp'), may hold values from -6 to 6
- w_gate: bfloat16 [8, 2816, 2048], P('sp', 'tp'), may hold values from -0.125 to 0.125
- w_up: bfloat16 [8, 2816, 2048], P('sp', 'tp'), may hold values from -0.125 to 0.125
- w_down: bfloat16 [8, 2816, 2048], P('sp', 'tp'), may hold values from -0.109375 to 0.109375
- conv_u: bfloat16 [1536, 512], P('sp', 'tp'), may hold values from -6 to 6
- conv_b: bfloat16 [1536, 512], P('sp', 'tp'), may hold values from -6 to 6
- conv_c: bfloat16 [1536, 512], P('sp', 'tp'), may hold values from -6 to 6
- conv_taps: float32 [3, 512], P(None, 'tp'), may hold values from -3 to 3
- out_proj: bfloat16 [512, 2048], P('tp'), may hold values from -0.25 to 0.25
Outputs:
- grad_w_gate: bfloat16 [8, 2816, 2048], P('sp', 'tp')
- grad_w_up: bfloat16 [8, 2816, 2048], P('sp', 'tp')
- grad_w_down: bfloat16 [8, 2816, 2048], P('sp', 'tp')
- grad_input: bfloat16 [1536, 2048], P('sp', 'tp')
- grad_proj: float32 [2048, 512], P('sp', 'tp')
- grad_u: bfloat16 [1536, 512], P('sp', 'tp')
- grad_b: bfloat16 [1536, 512], P('sp', 'tp')
- grad_c: bfloat16 [1536, 512], P('sp', 'tp')
The draws below stay inside these ranges and needn't reach their ends.
Inputs may be any that keep to these rules, and one draw needn't show every extreme that they name: `routes`: each row names two different experts. In each aligned block of 192 rows no expert is named more than 72 times, a bound that some block reaches.
All inputs are finite; a program needn't handle non-finite values.
Results may differ from the reference program's by a relative error of at most 0.025.
Values may be sent and summed in bfloat16 or wider, within the bound.
A program may use at most 64 MiB of HBM per device.

```python
import math
import jax
import jax.numpy as jnp
import numpy as np
from jax import lax

D = 2048
FF = 2816
CONV_W = 512
TOK_DEV = 192
EXPERTS = 8
CAP = 72
TOKENS = 1536
N_SP = 8
N_TP = 4


def raised(result, stream_key, source, target, blocks, factor):
    def block_of(dim):
        return (jnp.arange(result.shape[dim]) // (result.shape[dim] // blocks)).reshape((-1,) + (1,) * (result.ndim - 1 - dim))

    first = jax.random.permutation(stream_key, blocks)[block_of(target)]
    far = (block_of(target) + blocks // 2) % blocks
    return jnp.where((block_of(source) == first) | (block_of(source) == far), factor * result, result)


def steps_of(stream_key, shape, split, least, high):
    factor_of = 1.0
    for dim, shards_of in split:
        steps = jax.random.uniform(jax.random.fold_in(jax.random.fold_in(stream_key, 6), dim), (shards_of,), jnp.float32, least / len(split), high / len(split))
        factor_of = factor_of * jnp.repeat(jnp.exp(steps), shape[dim] // shards_of).reshape((-1,) + (1,) * (len(shape) - 1 - dim))
    return factor_of


def assign_block(own_key, own, number, rows, count, top, limit, slope):
    sequence = jax.random.permutation(own_key, count)
    packed, usual = shares(count, rows * top, limit, slope, True), shares(count, rows * top, limit, slope, False)
    places = jnp.arange(count)

    def named(tallies, offset_by):
        used = int((tallies > 0).sum())
        fixed = max(1, used // 4)
        passed = fixed + (places - fixed + offset_by * (used - fixed)) % max(1, count - fixed)
        return jnp.zeros((count,), jnp.int32).at[sequence[jnp.where(places < fixed, places, passed)]].set(jnp.asarray(tallies, jnp.int32))

    tallies = jnp.where(number % 4 == 0, named(packed, number // 4), named(usual, number - number // 4 - 1))
    mixed = jax.random.permutation(jax.random.fold_in(own, 3), count)
    giver, receiver = mixed[0:count // 2 * 2:2], mixed[1:count // 2 * 2:2]
    margin = jnp.minimum(tallies[giver] - 1, limit - tallies[receiver]) // 2
    margin = jnp.where((giver == sequence[0]) | (receiver == sequence[0]) | (tallies[receiver] == 0), 0, jnp.maximum(margin, 0))
    passed = jax.random.randint(jax.random.fold_in(own, 4), (count // 2,), 0, 1 << 20) % (margin + 1)
    tallies = tallies.at[giver].add(-passed).at[receiver].add(passed)
    items = jnp.searchsorted(jnp.cumsum(tallies), jnp.arange(rows * top), side="right").astype(jnp.int32)
    listing = items.reshape(top, rows).T
    listing = listing[jax.random.permutation(jax.random.fold_in(own, 1), rows)]
    offset_by = jax.random.randint(jax.random.fold_in(own, 2), (rows, 1), 0, top)
    return jnp.take_along_axis(listing, (jnp.arange(top)[None, :] + offset_by) % top, axis=1)


def shares(number_of, total, limit, skew, full):
    portions = [(1 << 20) // math.isqrt(standing ** skew) + 1 for standing in range(1, number_of + 1)]
    largest = limit if full else min(limit, max(-(-total // number_of), total * portions[0] // sum(portions)))
    least = 1 if total - largest >= number_of - 1 else 0
    counts, spare = [largest] + [least] * (number_of - 1), total - largest - least * (number_of - 1)
    while spare > 0:
        movable = [i for i in range(1, number_of) if counts[i] < largest] or [i for i in range(1, number_of) if counts[i] < limit]
        whole, remaining = sum([portions[i] for i in movable]), spare
        for i in movable:
            more = min(limit - counts[i], max(1, remaining * portions[i] // whole), spare)
            counts[i] = counts[i] + more
            spare = spare - more
    return np.array(counts)


def centred(key, dims, scale, reach, pieces=(), kind=jnp.bfloat16):
    level = steps_of(key, dims, pieces, -0.22, 0.18) if pieces else 1.0
    array = jax.random.normal(key, dims, jnp.float32) * scale * level
    return jnp.minimum(jnp.maximum(array, -reach), reach).astype(kind)


def heavy_noise(stream_key, shape, scale, bound, pieces, heavy, held_as=jnp.bfloat16):
    result = scale * jax.random.normal(stream_key, shape, jnp.float32)
    if pieces:
        result = result * steps_of(stream_key, shape, pieces, -0.22, 0.18)
    return jnp.clip(raised(result, jax.random.fold_in(stream_key, 3), *heavy), -bound, bound).astype(held_as)


def setup_inputs(seed: int = 0) -> dict:
    key_of = jax.random.split(jax.random.key(seed), 13)
    routes_keys = jax.random.split(jax.random.fold_in(key_of[0], 1), TOKENS // TOK_DEV)
    routes_turns = jax.random.permutation(jax.random.fold_in(key_of[0], 3), TOKENS // TOK_DEV)
    routes = jax.vmap(lambda own, number: assign_block(jax.random.fold_in(key_of[0], 2), own, number, TOK_DEV, EXPERTS, 2, CAP, 1))(routes_keys, routes_turns).reshape((TOKENS, 2))
    route_weights = jnp.clip(0.2 + 0.8 * jax.random.uniform(key_of[1], (TOKENS, 2), jnp.float32) ** steps_of(key_of[1], (TOKENS, 2), ((0, 8),), -0.2, 0.2), 0.2, 1.0)
    expert_inputs = centred(key_of[2], (TOKENS, D), 1.0, 6.0, ((0, 8), (1, 4)))
    out_grad = heavy_noise(key_of[3], (TOKENS, D), 1.0, 6.0, ((0, 8), (1, 4)), (0, 1, 8, 2.0))
    w_gate = centred(key_of[4], (EXPERTS, FF, D), D ** -0.5, 0.125, ((0, 8), (1, 4)))
    w_up = centred(key_of[5], (EXPERTS, FF, D), D ** -0.5, 0.125, ((0, 8), (1, 4)))
    w_down = centred(key_of[6], (EXPERTS, FF, D), FF ** -0.5, 0.109375, ((0, 8), (1, 4)))
    conv_u = centred(key_of[7], (TOKENS, CONV_W), 1.0, 6.0, ((0, 8), (1, 4)))
    conv_b = centred(key_of[8], (TOKENS, CONV_W), 1.0, 6.0, ((0, 8), (1, 4)))
    conv_c = centred(key_of[9], (TOKENS, CONV_W), 1.0, 6.0, ((0, 8), (1, 4)))
    conv_taps = centred(key_of[10], (3, CONV_W), 0.6, 3.0, ((1, 4),), jnp.float32)
    out_proj = centred(key_of[11], (CONV_W, D), CONV_W ** -0.5, 0.25, ((0, 4),))
    return {"routes": routes, "route_weights": route_weights, "expert_inputs": expert_inputs, "out_grad": out_grad, "w_gate": w_gate, "w_up": w_up, "w_down": w_down, "conv_u": conv_u, "conv_b": conv_b, "conv_c": conv_c, "conv_taps": conv_taps, "out_proj": out_proj}


def contract_first(left, right):
    return lax.dot_general(left, right, (((0,), (0,)), ((), ())), preferred_element_type=jnp.float32)


def contract_last(left, right):
    return lax.dot_general(left, right, (((1,), (1,)), ((), ())), preferred_element_type=jnp.float32)


def slot_tables(routes, capacity, experts):
    flat_expert = routes.reshape(-1).astype(jnp.int32)
    columns = lax.broadcasted_iota(jnp.int32, (flat_expert.shape[0], experts), 1)
    onehot = (flat_expert[:, None] == columns).astype(jnp.int32)
    before = jnp.cumsum(onehot, axis=0) - onehot
    slot_rank = jnp.sum(before * onehot, axis=1)
    slot_index = flat_expert * capacity + slot_rank
    labels = jnp.arange(flat_expert.shape[0], dtype=jnp.int32) + 1
    slot_owner = jnp.zeros((experts * capacity,), jnp.int32).at[slot_index].set(labels)
    return slot_index, slot_owner


def expert_backward(rows, grads, gate_weight, up_weight, down_weight):
    gate_pre = contract_last(rows, gate_weight)
    up_pre = contract_last(rows, up_weight)
    gate_act = jax.nn.silu(gate_pre)
    hidden = (gate_act * up_pre).astype(jnp.bfloat16)
    grad_down = contract_first(hidden, grads).astype(jnp.bfloat16)
    grad_hidden = contract_last(grads, down_weight)
    sigma = jax.nn.sigmoid(gate_pre)
    gate_back = (grad_hidden * up_pre * sigma * (1.0 + gate_pre * (1.0 - sigma))).astype(jnp.bfloat16)
    up_back = (grad_hidden * gate_act).astype(jnp.bfloat16)
    grad_gate = contract_first(gate_back, rows).astype(jnp.bfloat16)
    grad_up = contract_first(up_back, rows).astype(jnp.bfloat16)
    return grad_gate, grad_up, grad_down, gate_back, up_back


def reference(routes, route_weights, expert_inputs, out_grad, w_gate, w_up, w_down, conv_u, conv_b, conv_c, conv_taps, out_proj):
    f32 = jnp.float32
    bf16 = jnp.bfloat16
    scaled = (route_weights[:, :, None] * out_grad.astype(f32)[:, None, :]).astype(bf16).reshape(2 * TOKENS, D)
    repeated = jnp.repeat(expert_inputs, 2, axis=0)
    slot_index, slot_owner = jax.vmap(lambda block: slot_tables(block, CAP, EXPERTS))(routes.reshape(N_SP, TOK_DEV, 2))
    offsets = jnp.arange(N_SP, dtype=jnp.int32)[:, None] * (2 * TOK_DEV)
    filled = slot_owner > 0
    sources = jnp.where(filled, slot_owner - 1 + offsets, 0).astype(jnp.int32)

    def rearrange(table):
        return table.reshape(N_SP, EXPERTS, CAP).transpose(1, 0, 2).reshape(EXPERTS, N_SP * CAP)

    sources = rearrange(sources)
    filled = rearrange(filled)
    width = FF // N_TP

    def per_expert(expert):
        picked = sources[expert]
        mask = filled[expert][:, None]
        rows = jnp.where(mask, repeated[picked], jnp.zeros((), bf16))
        grads = jnp.where(mask, scaled[picked], jnp.zeros((), bf16))
        gate_weight = w_gate[expert]
        up_weight = w_up[expert]
        grad_gate, grad_up, grad_down, gate_back, up_back = expert_backward(rows, grads, gate_weight, up_weight, w_down[expert])
        count = rows.shape[0]
        partial_value = jnp.einsum("rnf,nfd->nrd", gate_back.astype(f32).reshape(count, N_TP, width), gate_weight.astype(f32).reshape(N_TP, width, D), precision=lax.Precision.HIGHEST)
        partial_value = partial_value + jnp.einsum("rnf,nfd->nrd", up_back.astype(f32).reshape(count, N_TP, width), up_weight.astype(f32).reshape(N_TP, width, D), precision=lax.Precision.HIGHEST)
        rounded = lax.optimization_barrier(partial_value.astype(bf16))
        back_rows = jnp.sum(rounded.astype(f32), axis=0).astype(bf16)
        return grad_gate, grad_up, grad_down, back_rows

    grad_w_gate, grad_w_up, grad_w_down, back_rows = lax.map(per_expert, jnp.arange(EXPERTS, dtype=jnp.int32))
    expert_of = routes.reshape(N_SP, 2 * TOK_DEV).astype(jnp.int32)
    slot_rank = slot_index - expert_of * CAP
    position = expert_of * (N_SP * CAP) + jnp.arange(N_SP, dtype=jnp.int32)[:, None] * CAP + slot_rank
    returned = back_rows.reshape(EXPERTS * N_SP * CAP, D)[position.reshape(-1)].astype(f32).reshape(TOKENS, 2, D)
    grad_input = (out_grad.astype(f32) + returned[:, 0] + returned[:, 1]).astype(bf16)

    length = TOKENS
    mixed_in = conv_c.astype(f32) * conv_u.astype(f32)
    padded = jnp.pad(mixed_in, ((1, 1), (0, 0)))
    convolved = conv_taps[0] * padded[0:length] + conv_taps[1] * padded[1:length + 1] + conv_taps[2] * padded[2:length + 2]
    conv_out = (conv_b.astype(f32) * convolved).astype(bf16)
    grad_conv = contract_last(grad_input, out_proj)
    grad_proj = contract_first(grad_input, conv_out)
    grad_b = (grad_conv * convolved).astype(bf16)
    grad_mixed = grad_conv * conv_b.astype(f32)
    rim = jnp.pad(grad_mixed, ((1, 1), (0, 0)))
    grad_z = conv_taps[0] * rim[2:length + 2] + conv_taps[1] * rim[1:length + 1] + conv_taps[2] * rim[0:length]
    grad_c = (grad_z * conv_u.astype(f32)).astype(bf16)
    grad_u = (grad_z * conv_c.astype(f32)).astype(bf16)
    return grad_w_gate, grad_w_up, grad_w_down, grad_input, grad_proj, grad_u, grad_b, grad_c
```

```python
import functools

import jax
import jax.numpy as jnp
from jax import lax
from jax.experimental import pallas as pl
from jax.experimental.pallas import tpu as pltpu
from jax.sharding import PartitionSpec as P

MESH = pl.DeviceIdType.MESH
F32 = jnp.float32
BF16 = jnp.bfloat16


def contract_first(left, right):
    return lax.dot_general(
        left, right, (((0,), (0,)), ((), ())), preferred_element_type=jnp.float32
    )


def contract_last(left, right):
    return lax.dot_general(
        left, right, (((1,), (1,)), ((), ())), preferred_element_type=jnp.float32
    )


def loop(count, step):
    lax.fori_loop(0, count, lambda i, c: (step(i), c)[1], 0)


def enter(sizes):
    barrier = pltpu.get_barrier_semaphore()
    for axis, size in sizes:
        me = lax.axis_index(axis)

        def greet(i, axis=axis, size=size, me=me):
            pl.semaphore_signal(
                barrier,
                inc=1,
                device_id={axis: lax.rem(me + i + 1, size)},
                device_id_type=MESH,
            )

        loop(size - 1, greet)
    return lambda: pl.semaphore_wait(barrier, sum(size - 1 for _, size in sizes))


def remote(src, dst, send, recv, **where):
    return pltpu.make_async_remote_copy(
        src_ref=src,
        dst_ref=dst,
        send_sem=send,
        recv_sem=recv,
        device_id=where,
        device_id_type=MESH,
    )


def slot_codes(routes, experts):
    count = routes.shape[1]
    names = lax.broadcasted_iota(jnp.int32, (experts, count), 0)
    first = (routes[0:1, :] == names).astype(F32)
    second = (routes[1:2, :] == names).astype(F32)
    early = lax.broadcasted_iota(jnp.int32, (count, count), 0)
    late = lax.broadcasted_iota(jnp.int32, (count, count), 1)
    before = (early < late).astype(F32).astype(BF16)
    rank = jnp.dot((first + second).astype(BF16), before, preferred_element_type=F32)
    code = jnp.where(first + second > 0.5, rank, -1.0).astype(jnp.int32)
    return code, first, second


def padded_rows(cap):
    return -(-cap // 16) * 16


def expert_kernel(
    S, T, routes_ref, wts_ref, xin_ref, gin_ref, edge_ref, gate_hbm, up_hbm, down_hbm,
    own_ref, full_ref, halo_ref, dgate_ref, dup_ref, ddown_ref,
    gate_w, up_w, down_w, code_ref, weight_ref, zs, xg, xc, pre, upre,
    hid, gback, uback, hid_t, gback_t, uback_t, part, landed, met, passed, summed, back, total_ref,
    wsem, zsend, zrecv, fsend, frecv, rsend, rrecv,
    tsend, trecv, bsend, brecv, ysend, yrecv, asend, arecv, hsend, hrecv,
):
    s, p = lax.axis_index("sp"), lax.axis_index("tp")
    n = S // 2
    z, c = s // 2, lax.rem(s, 2)
    cap, d = summed.shape[1], summed.shape[2]
    capp = padded_rows(cap)
    half = d // 2
    relay = T == 4
    wait_entry = enter((("sp", S), ("tp", T)))

    weights = [
        pltpu.make_async_copy(src.at[0], dst, wsem.at[i])
        for i, (src, dst) in enumerate(((gate_hbm, gate_w), (up_hbm, up_w), (down_hbm, down_w)))
    ]
    for w in weights:
        w.start()

    def offset(q):
        odd = lax.rem(q, 2)
        return lax.rem(odd * ((q + 1) // 2) + (1 - odd) * (n - q // 2), n)

    def dest(j):
        return 2 * lax.rem(z + offset(j // 2), n) + lax.rem(c + j, 2)

    def origin(j):
        return 2 * lax.rem(z - offset(j // 2) + n, n) + lax.rem(c + j, 2)

    def cols(q):
        return pl.ds(pl.multiple_of(q * d, d), d)

    def halfcols(q, h):
        return pl.ds(pl.multiple_of(q * d + h * half, half), half)

    if relay:
        xn, yn = p + 1 - 2 * lax.rem(p, 2), lax.rem(p + 2, 4)
        partners = ((xn, xn), (yn, yn))
        order = ((xn, yn), (yn, xn))
    else:
        xn, yn = p, p
        partners = tuple(
            (lax.rem(p + r, T), lax.rem(p - r + T, T)) for r in range(1, T)
        )

    code, first, second = slot_codes(routes_ref[...], S)
    code_ref[...] = code
    weight_ref[...] = first * wts_ref[0:1, :] + second * wts_ref[1:2, :]
    slots = lax.broadcasted_iota(jnp.int32, (cap, code.shape[1]), 0)

    def pick(j):
        to = dest(j)
        mask = slots == code_ref[pl.ds(to, 1), :]
        chosen = mask.astype(F32).astype(BF16)
        zs[0, to] = jnp.dot(chosen, xin_ref[...], preferred_element_type=F32).astype(BF16)
        held = jnp.sum(
            jnp.where(mask, weight_ref[pl.ds(to, 1), :], 0.0), axis=1, keepdims=True
        )
        zs[1, to] = (held * jnp.dot(chosen, gin_ref[...], preferred_element_type=F32)).astype(BF16)

    def zcopy(i, j, arriving=False):
        to = dest(j)
        row = origin(j) if arriving else s
        return remote(
            zs.at[i, to], xg.at[i, row, :, cols(p)], zsend.at[i, j], zrecv.at[i, j], sp=to
        )

    def fcopy(i, j, k, arriving=False):
        to, whence = partners[k]
        view = xg.at[i, origin(j), :, cols(whence if arriving else p)]
        return remote(view, view, fsend.at[i, j, k], frecv.at[i, j, k], tp=to)

    def rcopy(i, j, k, arriving=False):
        near, far = ((xn, yn), (yn, xn))[k]
        view = xg.at[i, origin(j), :, halfcols(3 - p if arriving else near, k)]
        return remote(view, view, rsend.at[i, j, k], rrecv.at[i, j, k], tp=far)

    def spread(i, j):
        for k in range(len(partners)):
            fcopy(i, j, k).start()

    def forward(i, j):
        zcopy(i, j, True).wait_recv()
        spread(i, j)

    def pass_on(i, j):
        for k in range(len(partners)):
            fcopy(i, j, k, True).wait_recv()
            if relay:
                rcopy(i, j, k).start()

    def ready(i, q):
        for b in range(2):
            j = 2 * q + b
            if relay:
                for k in range(2):
                    rcopy(i, j, k, True).wait_recv()
            xc[i, pl.ds(pl.multiple_of(j * capp, capp), cap), :] = xg[i, origin(j)]

    def zback(j, arriving=False):
        row = dest(j) if arriving else s
        return remote(
            summed.at[j], back.at[row], ysend.at[j], yrecv.at[j], sp=origin(j)
        )

    if relay:

        def tcopy(j, h, k):
            to = order[h][0]
            return remote(
                part.at[j, :, halfcols(3 - p if k else to, h)],
                landed.at[h, k, j],
                tsend.at[j, 2 * h + k],
                trecv.at[j, 2 * h + k],
                tp=to,
            )

        def bcopy(j, h):
            return remote(
                passed.at[h, j], met.at[h, j], bsend.at[j, h], brecv.at[j, h], tp=order[h][1]
            )

        def give(j):
            for k in (1, 0):
                for h in range(2):
                    tcopy(j, h, k).start()

        def combine(j):
            for h in range(2):
                tcopy(j, h, 1).wait_recv()
                mine = part[j, :, halfcols(order[h][1], h)].astype(F32)
                passed[h, j] = (mine + landed[h, 1, j].astype(F32)).astype(BF16)

        def total(j, out, row):
            for h in range(2):
                tcopy(j, h, 0).wait_recv()
                bcopy(j, h).wait_recv()
                mine = part[j, :, halfcols(p, h)].astype(F32)
                mine = mine + landed[h, 0, j].astype(F32)
                mine = mine + met[h, j].astype(F32)
                out[row, :, h * half : (h + 1) * half] = mine.astype(BF16)

    else:

        def tcopy(j, r):
            q = lax.rem(p + r, T)
            return remote(
                part.at[j, :, cols(q)],
                landed.at[r - 1, j],
                tsend.at[j, r - 1],
                trecv.at[j, r - 1],
                tp=q,
            )

        def give(j):
            for r in range(1, T):
                tcopy(j, r).start()

        def total(j, out, row):
            for r in range(1, T):
                tcopy(j, r).wait_recv()
            value = part[j, :, cols(p)].astype(F32)
            for r in range(1, T):
                value = value + landed[r - 1, j].astype(F32)
            out[row] = value.astype(BF16)

    lag = 2

    def block(r):
        return lax.rem(r + 2, S)

    def service(t):
        if relay:

            @pl.when(t < S)
            def _():
                combine(block(t))

        @pl.when(jnp.logical_and(jnp.logical_and(t >= lag, t < S + lag), t - lag != S - 2))
        def _():
            total(block(t - lag), summed, block(t - lag))

        @pl.when(t - lag == S - 2)
        def _():
            total(0, back, s)

        if relay:

            @pl.when(t < S)
            def _():
                for h in range(2):
                    bcopy(block(t), h).start()

        @pl.when(jnp.logical_and(t >= lag + 1, t - lag - 1 != S - 2))
        def _():
            zback(block(t - lag - 1)).start()

    def give_chunk(q):
        give(2 * q)
        give(2 * q + 1)

    pick(0)
    xg[0, s, :, cols(p)] = zs[0, s]
    xg[1, s, :, cols(p)] = zs[1, s]
    pick(1)
    xc[...] = jnp.zeros_like(xc)
    wait_entry()
    for i in range(2):
        spread(i, 0)

    def send_picked(k):
        @pl.when(k + 2 < S)
        def _():
            pick(k + 2)

        for i in range(2):
            zcopy(i, k + 1).start()

    loop(S - 1, send_picked)

    def hcopy(k):
        to = lax.rem(s + (1 if k == 0 else S - 1), S)
        return remote(
            edge_ref.at[1 - k], halo_ref.at[k], hsend.at[k], hrecv.at[k], sp=to
        )

    for k in range(2):
        hcopy(k).start()

    def chunk(q):
        return pl.ds(pl.multiple_of(q * 2 * capp, 2 * capp), 2 * capp)

    def step(q):
        live, later, last = q < n, q > 0, q == n

        @pl.when(jnp.logical_and(live, later))
        def _():
            forward(0, 2 * q)

        @pl.when(later)
        def _():
            pass_on(1, 2 * q - 1)

        @pl.when(last)
        def _():
            give_chunk(n - 2)
            service(0)

        @pl.when(later)
        def _():
            ready(0, q - 1)

            @pl.when(q == 1)
            def _():
                for w in weights:
                    w.wait()

            pre[...] = contract_last(xc[0, chunk(q - 1), :], gate_w[...])

        @pl.when(live)
        def _():
            forward(0, 2 * q + 1)
            pass_on(0, 2 * q)

        @pl.when(last)
        def _():
            service(1)

        @pl.when(later)
        def _():
            upre[...] = contract_last(xc[0, chunk(q - 1), :], up_w[...])

        @pl.when(jnp.logical_and(live, later))
        def _():
            forward(1, 2 * q)

        @pl.when(live)
        def _():
            pass_on(0, 2 * q + 1)

        @pl.when(last)
        def _():
            service(2)

        @pl.when(later)
        def _():
            ready(1, q - 1)
            grad_hidden = contract_last(xc[1, chunk(q - 1), :], down_w[...])
            gate_pre, up_pre = pre[...], upre[...]
            sigma = jax.nn.sigmoid(gate_pre)
            gate_act = gate_pre * sigma
            hid[chunk(q - 1), :] = (gate_act * up_pre).astype(BF16)
            gback[chunk(q - 1), :] = (
                grad_hidden * up_pre * sigma * (1.0 + gate_pre * (1.0 - sigma))
            ).astype(BF16)
            uback[chunk(q - 1), :] = (grad_hidden * gate_act).astype(BF16)

        @pl.when(live)
        def _():
            forward(1, 2 * q + 1)
            pass_on(1, 2 * q)

        @pl.when(last)
        def _():
            service(3)

        @pl.when(later)
        def _():
            def piece(f):
                value = jnp.dot(
                    gback[chunk(q - 1), :], gate_w[:, cols(f)], preferred_element_type=F32
                ) + jnp.dot(
                    uback[chunk(q - 1), :], up_w[:, cols(f)], preferred_element_type=F32
                )
                for b in range(2):
                    part[2 * (q - 1) + b, :, cols(f)] = value[
                        b * capp : b * capp + cap
                    ].astype(BF16)

            loop(T, piece)

        @pl.when(q == n - 1)
        def _():
            loop(n - 3, lambda k: give_chunk(k + 1))

        @pl.when(last)
        def _():
            give_chunk(n - 1)
            give_chunk(0)

    loop(n + 1, step)

    hid_t[...] = hid[...].T
    gback_t[...] = gback[...].T
    uback_t[...] = uback[...].T
    jobs = ((hid_t, 1, ddown_ref), (gback_t, 0, dgate_ref), (uback_t, 0, dup_ref))
    width = 512
    tiles = T * d // width

    def weight_piece(k):
        for which, (left, i, out) in enumerate(jobs):

            @pl.when(k // tiles == which)
            def _(left=left, i=i, out=out):
                at = pl.ds(pl.multiple_of(lax.rem(k, tiles) * width, width), width)
                out[:, at] = jnp.dot(
                    left[...], xc[i, :, at], preferred_element_type=F32
                ).astype(BF16)

    steps = S + lag + 1 - 4
    each = -(-3 * tiles // (steps - 1))

    def finish_step(t):
        for k in range(each):

            @pl.when(t * each + k < 3 * tiles)
            def _(k=k):
                weight_piece(t * each + k)

        service(t + 4)

    loop(steps, finish_step)

    total_ref[...] = gin_ref[...].astype(F32)

    def gathered(r):
        j = block(r)
        at = dest(j)

        @pl.when(j != 0)
        def _():
            zback(j, True).wait_recv()

        chosen = (slots == code_ref[pl.ds(at, 1), :]).astype(F32).astype(BF16)
        total_ref[...] += contract_first(chosen, back[at])

    loop(S, gathered)
    value = total_ref[...].astype(BF16)
    own_ref[...] = value
    full_ref[:, cols(p)] = value

    def acopy(r, arriving=False):
        at = lax.rem(p - r + T, T) if arriving else p
        return remote(
            own_ref, full_ref.at[:, cols(at)], asend.at[r - 1], arecv.at[r - 1],
            tp=lax.rem(p + r, T),
        )

    loop(S - 1, lambda k: zback(k + 1).wait_send())
    for r in range(1, T):
        acopy(r).start()

    def drain(j):
        for i in range(2):

            @pl.when(j > 0)
            def _(i=i):
                zcopy(i, j).wait_send()

            for k in range(len(partners)):
                fcopy(i, j, k).wait_send()
                if relay:
                    rcopy(i, j, k).wait_send()
        if relay:
            for h in range(2):
                tcopy(j, h, 0).wait_send()
                tcopy(j, h, 1).wait_send()
                bcopy(j, h).wait_send()
        else:
            for r in range(1, T):
                tcopy(j, r).wait_send()

    loop(S, drain)
    for k in range(2):
        hcopy(k).wait()
    for r in range(1, T):
        acopy(r).wait_send()
        acopy(r, True).wait_recv()


def finish_kernel(
    dgate, dup, ddown, own_ref, sum_ref, dgate_out, dup_out, ddown_out, own_out, sum_out, sem
):
    copies = [
        pltpu.make_async_copy(src, dst, sem.at[i])
        for i, (src, dst) in enumerate(((dgate, dgate_out), (dup, dup_out), (ddown, ddown_out)))
    ]
    for copy in copies:
        copy.start()
    own_out[...] = own_ref[...]
    sum_out[...] = sum_ref[...]
    for copy in copies:
        copy.wait()


def reduce_kernel(
    S, proj_ref, edge_ref, sum_ref, halo_ref,
    given, pairs, landed, gsend, grecv, psend, precv, hsend, hrecv,
):
    s = lax.axis_index("sp")
    n = S // 2
    z, c = s // 2, lax.rem(s, 2)
    enter((("sp", S),))()

    def hcopy(k):
        to = lax.rem(s + (1 if k == 0 else S - 1), S)
        return remote(
            edge_ref.at[1 - k], halo_ref.at[k], hsend.at[k], hrecv.at[k], sp=to
        )

    def at(o):
        return lax.rem(z + o, n)

    def gcopy(o):
        return remote(
            proj_ref.at[2 * at(o) + 1 - c], given.at[at(o)],
            gsend.at[o], grecv.at[o], sp=s + 1 - 2 * c,
        )

    def pcopy(o):
        return remote(
            pairs.at[at(o)], landed.at[o - 1], psend.at[o - 1], precv.at[o - 1],
            sp=2 * at(o) + c,
        )

    for k in range(2):
        hcopy(k).start()
    for o in range(1, n + 1):
        gcopy(o % n).start()

    def pair(o):
        gcopy(o).wait_recv()
        return proj_ref[2 * at(o) + c].astype(F32) + given[at(o)].astype(F32)

    for o in range(1, n):
        pairs[at(o)] = pair(o).astype(BF16)
        if o > 1:
            pcopy(o - 1).start()
    sum_ref[...] = pair(0)
    pcopy(n - 1).start()
    for o in range(1, n):
        pcopy(o).wait_recv()
        sum_ref[...] += landed[o - 1].astype(F32)
    for o in range(n):
        gcopy(o).wait_send()
        if o > 0:
            pcopy(o).wait_send()
    for k in range(2):
        hcopy(k).wait()


def vmem(count):
    return [pl.BlockSpec(memory_space=pltpu.VMEM)] * count


def params(number):
    return pltpu.CompilerParams(
        collective_id=number, has_side_effects=True, vmem_limit_bytes=16 * 2**20
    )


def rimmed(value, halo):
    s, size = lax.axis_index("sp"), lax.axis_size("sp")
    before = jnp.where(s > 0, halo[0, -1:], 0.0)
    after = jnp.where(s < size - 1, halo[1, :1], 0.0)
    return jnp.concatenate([before, value, after], axis=0)


def edges(value):
    return jnp.stack([value[:8], value[-8:]])


def body(
    routes, route_weights, expert_inputs, out_grad, w_gate, w_up, w_down,
    conv_u, conv_b, conv_c, conv_taps, out_proj,
):
    S, T = lax.axis_size("sp"), lax.axis_size("tp")
    tokens, d = expert_inputs.shape
    channels = conv_u.shape[1]
    cap = 3 * tokens // S
    capp = padded_rows(cap)
    hidden = w_gate.shape[1]
    dma = pltpu.SemaphoreType.DMA
    ways = 2 if T == 4 else T - 1
    relays = (2, S, 2) if T == 4 else (1, 1, 1)
    if T == 4:
        pieces = 4
        shapes = ((2, 2, S, cap, d // 2), (2, S, cap, d // 2), (2, S, cap, d // 2))
    else:
        pieces = T - 1
        shapes = ((T - 1, S, cap, d), (8, 128), (8, 128))
    landing = [pltpu.VMEM(shape, BF16) for shape in shapes]
    mixed_in = conv_c.astype(F32) * conv_u.astype(F32)
    halo_shape = jax.ShapeDtypeStruct((2, 8, channels), F32)
    grad_w = jax.ShapeDtypeStruct((hidden, T * d), BF16)
    anywhere = pl.BlockSpec(memory_space=pl.ANY)
    grad_input, grad_full, halo, grad_gate, grad_up, grad_down = pl.pallas_call(
        functools.partial(expert_kernel, S, T),
        out_shape=(
            jax.ShapeDtypeStruct((tokens, d), BF16),
            jax.ShapeDtypeStruct((tokens, T * d), BF16),
            halo_shape,
            grad_w,
            grad_w,
            grad_w,
        ),
        in_specs=vmem(5) + [anywhere] * 3,
        out_specs=tuple(vmem(6)),
        scratch_shapes=[
            pltpu.VMEM((hidden, T * d), BF16),
            pltpu.VMEM((hidden, T * d), BF16),
            pltpu.VMEM((hidden, T * d), BF16),
            pltpu.VMEM((S, tokens), jnp.int32),
            pltpu.VMEM((S, tokens), F32),
            pltpu.VMEM((2, S, cap, d), BF16),
            pltpu.VMEM((2, S, cap, T * d), BF16),
            pltpu.VMEM((2, S * capp, T * d), BF16),
            pltpu.VMEM((2 * capp, hidden), F32),
            pltpu.VMEM((2 * capp, hidden), F32),
            pltpu.VMEM((S * capp, hidden), BF16),
            pltpu.VMEM((S * capp, hidden), BF16),
            pltpu.VMEM((S * capp, hidden), BF16),
            pltpu.VMEM((hidden, S * capp), BF16),
            pltpu.VMEM((hidden, S * capp), BF16),
            pltpu.VMEM((hidden, S * capp), BF16),
            pltpu.VMEM((S, cap, T * d), BF16),
            *landing,
            pltpu.VMEM((S, cap, d), BF16),
            pltpu.VMEM((S, cap, d), BF16),
            pltpu.VMEM((tokens, d), F32),
            dma((3,)),
            dma((2, S)),
            dma((2, S)),
            dma((2, S, ways)),
            dma((2, S, ways)),
            dma(relays),
            dma(relays),
            dma((S, pieces)),
            dma((S, pieces)),
            dma(relays[1:]),
            dma(relays[1:]),
            dma((S,)),
            dma((S,)),
            dma((T - 1,)),
            dma((T - 1,)),
            dma((2,)),
            dma((2,)),
        ],
        compiler_params=pltpu.CompilerParams(
            collective_id=0, has_side_effects=True, vmem_limit_bytes=56 * 2**20
        ),
        name="experts",
    )(
        routes.T, route_weights.T, expert_inputs, out_grad, edges(mixed_in),
        w_gate, w_up, w_down,
    )

    padded = rimmed(mixed_in, halo)
    convolved = (
        conv_taps[0] * padded[0:tokens]
        + conv_taps[1] * padded[1 : tokens + 1]
        + conv_taps[2] * padded[2 : tokens + 2]
    )
    conv_out = (conv_b.astype(F32) * convolved).astype(BF16)
    grad_conv = contract_last(grad_full, out_proj)
    grad_b = (grad_conv * convolved).astype(BF16)
    grad_mixed = grad_conv * conv_b.astype(F32)
    proj = contract_first(grad_full, conv_out).astype(BF16)
    width = proj.shape[0] // S
    proj_sum, halo = pl.pallas_call(
        functools.partial(reduce_kernel, S),
        out_shape=(jax.ShapeDtypeStruct((width, channels), F32), halo_shape),
        in_specs=vmem(2),
        out_specs=tuple(vmem(2)),
        scratch_shapes=[
            pltpu.VMEM((S // 2, width, channels), BF16),
            pltpu.VMEM((S // 2, width, channels), BF16),
            pltpu.VMEM((S // 2 - 1, width, channels), BF16),
            dma((S // 2,)),
            dma((S // 2,)),
            dma((S // 2 - 1,)),
            dma((S // 2 - 1,)),
            dma((2,)),
            dma((2,)),
        ],
        compiler_params=params(2),
        name="sum_proj",
    )(proj.reshape(S, width, channels), edges(grad_mixed))
    rim = rimmed(grad_mixed, halo)
    grad_z = (
        conv_taps[0] * rim[2 : tokens + 2]
        + conv_taps[1] * rim[1 : tokens + 1]
        + conv_taps[2] * rim[0:tokens]
    )
    grad_c = (grad_z * conv_u.astype(F32)).astype(BF16)
    grad_u = (grad_z * conv_c.astype(F32)).astype(BF16)
    grad_gate, grad_up, grad_down, grad_input, proj_sum = pl.pallas_call(
        finish_kernel,
        out_shape=tuple(
            jax.ShapeDtypeStruct(v.shape, v.dtype)
            for v in (grad_gate, grad_up, grad_down, grad_input, proj_sum)
        ),
        in_specs=vmem(5),
        out_specs=tuple([anywhere] * 3 + vmem(2)),
        scratch_shapes=[dma((3,))],
        compiler_params=pltpu.CompilerParams(vmem_limit_bytes=32 * 2**20),
        name="finish",
    )(grad_gate, grad_up, grad_down, grad_input, proj_sum)
    return (
        grad_gate[None], grad_up[None], grad_down[None], grad_input, proj_sum,
        grad_u, grad_b, grad_c,
    )


def solution(mesh):
    in_specs = (
        P("sp", None),
        P("sp", None),
        P("sp", "tp"),
        P("sp", "tp"),
        P("sp", "tp", None),
        P("sp", "tp", None),
        P("sp", "tp", None),
        P("sp", "tp"),
        P("sp", "tp"),
        P("sp", "tp"),
        P(None, "tp"),
        P("tp", None),
    )
    out_specs = (
        P("sp", "tp", None),
        P("sp", "tp", None),
        P("sp", "tp", None),
        P("sp", "tp"),
        P("sp", "tp"),
        P("sp", "tp"),
        P("sp", "tp"),
        P("sp", "tp"),
    )
    return jax.shard_map(body, mesh=mesh, in_specs=in_specs, out_specs=out_specs, check_vma=False)
```

```python
import functools

import jax
import jax.numpy as jnp
from jax import lax
from jax.experimental import pallas as pl
from jax.experimental.pallas import tpu as pltpu
from jax.sharding import PartitionSpec as P

MESH = pl.DeviceIdType.MESH
F32 = jnp.float32
BF16 = jnp.bfloat16


def contract_first(left, right):
    return lax.dot_general(
        left, right, (((0,), (0,)), ((), ())), preferred_element_type=jnp.float32
    )


def contract_last(left, right):
    return lax.dot_general(
        left, right, (((1,), (1,)), ((), ())), preferred_element_type=jnp.float32
    )


def loop(count, step):
    lax.fori_loop(0, count, lambda i, c: (step(i), c)[1], 0)


def enter(sizes):
    barrier = pltpu.get_barrier_semaphore()
    for axis, size in sizes:
        me = lax.axis_index(axis)

        def greet(i, axis=axis, size=size, me=me):
            pl.semaphore_signal(
                barrier,
                inc=1,
                device_id={axis: lax.rem(me + i + 1, size)},
                device_id_type=MESH,
            )

        loop(size - 1, greet)
    return lambda: pl.semaphore_wait(barrier, sum(size - 1 for _, size in sizes))


def remote(src, dst, send, recv, **where):
    return pltpu.make_async_remote_copy(
        src_ref=src,
        dst_ref=dst,
        send_sem=send,
        recv_sem=recv,
        device_id=where,
        device_id_type=MESH,
    )


def slot_codes(routes, experts):
    count = routes.shape[1]
    names = lax.broadcasted_iota(jnp.int32, (experts, count), 0)
    first = (routes[0:1, :] == names).astype(F32)
    second = (routes[1:2, :] == names).astype(F32)
    early = lax.broadcasted_iota(jnp.int32, (count, count), 0)
    late = lax.broadcasted_iota(jnp.int32, (count, count), 1)
    before = (early < late).astype(F32).astype(BF16)
    rank = jnp.dot((first + second).astype(BF16), before, preferred_element_type=F32)
    code = jnp.where(first + second > 0.5, rank, -1.0).astype(jnp.int32)
    return code, first, second


def padded_rows(cap):
    return -(-cap // 16) * 16


def expert_kernel(
    S, T, routes_hbm, wts_hbm, xin_hbm, gin_hbm, gate_hbm, up_hbm, down_hbm,
    u_hbm, b_hbm, c_hbm, taps_hbm, outw_hbm,
    own_ref, sum_ref, gu_ref, gb_ref, gc_ref, dgate_ref, dup_ref, ddown_ref,
    routes_ref, wts_ref, xin_ref, gin_ref, gate_w, up_w, down_w,
    u_ref, b_ref, c_ref, taps_ref, out_w,
    code_ref, weight_ref, zs, xg, xc, pre, upre,
    hid, gback, uback, hid_t, gback_t, uback_t, part, landed, met, passed, summed, back, total_ref,
    full_ref, edge_ref, halo_ref, rim, conv_ref, y_ref, dy_ref, proj, given, pairs, arrived,
    isem, zsend, zrecv, fsend, frecv, rsend, rrecv,
    tsend, trecv, bsend, brecv, ysend, yrecv, asend, arecv, hsend, hrecv,
    gsend, grecv, psend, precv,
):
    s, p = lax.axis_index("sp"), lax.axis_index("tp")
    n = S // 2
    z, c = s // 2, lax.rem(s, 2)
    cap, d = summed.shape[1], summed.shape[2]
    tokens = own_ref.shape[0]
    capp = padded_rows(cap)
    half = d // 2
    relay = T == 4
    wait_entry = enter((("sp", S), ("tp", T)))

    loads = [
        pltpu.make_async_copy(src, dst, isem.at[i])
        for i, (src, dst) in enumerate(
            (
                (routes_hbm, routes_ref), (wts_hbm, wts_ref), (xin_hbm, xin_ref),
                (gin_hbm, gin_ref), (u_hbm, u_ref), (c_hbm, c_ref), (gate_hbm.at[0], gate_w),
                (up_hbm.at[0], up_w), (down_hbm.at[0], down_w), (b_hbm, b_ref),
                (taps_hbm, taps_ref), (outw_hbm, out_w),
            )
        )
    ]
    for load in loads:
        load.start()
    for load in loads[:4]:
        load.wait()

    def offset(q):
        odd = lax.rem(q, 2)
        return lax.rem(odd * ((q + 1) // 2) + (1 - odd) * (n - q // 2), n)

    def dest(j):
        return 2 * lax.rem(z + offset(j // 2), n) + lax.rem(c + j, 2)

    def origin(j):
        return 2 * lax.rem(z - offset(j // 2) + n, n) + lax.rem(c + j, 2)

    def cols(q):
        return pl.ds(pl.multiple_of(q * d, d), d)

    def halfcols(q, h):
        return pl.ds(pl.multiple_of(q * d + h * half, half), half)

    if relay:
        xn, yn = p + 1 - 2 * lax.rem(p, 2), lax.rem(p + 2, 4)
        partners = ((xn, xn), (yn, yn))
        order = ((xn, yn), (yn, xn))
    else:
        xn, yn = p, p
        partners = tuple(
            (lax.rem(p + r, T), lax.rem(p - r + T, T)) for r in range(1, T)
        )

    code, first, second = slot_codes(routes_ref[...], S)
    code_ref[...] = code
    weight_ref[...] = first * wts_ref[0:1, :] + second * wts_ref[1:2, :]
    slots = lax.broadcasted_iota(jnp.int32, (cap, code.shape[1]), 0)

    def pick(j):
        to = dest(j)
        mask = slots == code_ref[pl.ds(to, 1), :]
        chosen = mask.astype(F32).astype(BF16)
        zs[0, to] = jnp.dot(chosen, xin_ref[...], preferred_element_type=F32).astype(BF16)
        held = jnp.sum(
            jnp.where(mask, weight_ref[pl.ds(to, 1), :], 0.0), axis=1, keepdims=True
        )
        zs[1, to] = (held * jnp.dot(chosen, gin_ref[...], preferred_element_type=F32)).astype(BF16)

    def zcopy(i, j, arriving=False):
        to = dest(j)
        row = origin(j) if arriving else s
        return remote(
            zs.at[i, to], xg.at[i, row, :, cols(p)], zsend.at[i, j], zrecv.at[i, j], sp=to
        )

    def fcopy(i, j, k, arriving=False):
        to, whence = partners[k]
        view = xg.at[i, origin(j), :, cols(whence if arriving else p)]
        return remote(view, view, fsend.at[i, j, k], frecv.at[i, j, k], tp=to)

    def rcopy(i, j, k, arriving=False):
        near, far = ((xn, yn), (yn, xn))[k]
        view = xg.at[i, origin(j), :, halfcols(3 - p if arriving else near, k)]
        return remote(view, view, rsend.at[i, j, k], rrecv.at[i, j, k], tp=far)

    def spread(i, j):
        for k in range(len(partners)):
            fcopy(i, j, k).start()

    def forward(i, j):
        zcopy(i, j, True).wait_recv()
        spread(i, j)

    def pass_on(i, j):
        for k in range(len(partners)):
            fcopy(i, j, k, True).wait_recv()
            if relay:
                rcopy(i, j, k).start()

    def ready(i, q):
        for b in range(2):
            j = 2 * q + b
            if relay:
                for k in range(2):
                    rcopy(i, j, k, True).wait_recv()
            xc[i, pl.ds(pl.multiple_of(j * capp, capp), cap), :] = xg[i, origin(j)]

    def zback(j, arriving=False):
        row = dest(j) if arriving else s
        return remote(
            summed.at[j], back.at[row], ysend.at[j], yrecv.at[j], sp=origin(j)
        )

    if relay:

        def tcopy(j, h, k):
            to = order[h][0]
            return remote(
                part.at[j, :, halfcols(3 - p if k else to, h)],
                landed.at[h, k, j],
                tsend.at[j, 2 * h + k],
                trecv.at[j, 2 * h + k],
                tp=to,
            )

        def bcopy(j, h):
            return remote(
                passed.at[h, j], met.at[h, j], bsend.at[j, h], brecv.at[j, h], tp=order[h][1]
            )

        def give(j):
            for k in (1, 0):
                for h in range(2):
                    tcopy(j, h, k).start()

        def combine(j):
            for h in range(2):
                tcopy(j, h, 1).wait_recv()
                mine = part[j, :, halfcols(order[h][1], h)].astype(F32)
                passed[h, j] = (mine + landed[h, 1, j].astype(F32)).astype(BF16)

        def total(j, out, row):
            for h in range(2):
                tcopy(j, h, 0).wait_recv()
                bcopy(j, h).wait_recv()
                mine = part[j, :, halfcols(p, h)].astype(F32)
                mine = mine + landed[h, 0, j].astype(F32)
                mine = mine + met[h, j].astype(F32)
                out[row, :, h * half : (h + 1) * half] = mine.astype(BF16)

    else:

        def tcopy(j, r):
            q = lax.rem(p + r, T)
            return remote(
                part.at[j, :, cols(q)],
                landed.at[r - 1, j],
                tsend.at[j, r - 1],
                trecv.at[j, r - 1],
                tp=q,
            )

        def give(j):
            for r in range(1, T):
                tcopy(j, r).start()

        def total(j, out, row):
            for r in range(1, T):
                tcopy(j, r).wait_recv()
            value = part[j, :, cols(p)].astype(F32)
            for r in range(1, T):
                value = value + landed[r - 1, j].astype(F32)
            out[row] = value.astype(BF16)

    lag = 2

    def block(r):
        return lax.rem(r + 2, S)

    def service(t):
        if relay:

            @pl.when(t < S)
            def _():
                combine(block(t))

        @pl.when(jnp.logical_and(jnp.logical_and(t >= lag, t < S + lag), t - lag != S - 2))
        def _():
            total(block(t - lag), summed, block(t - lag))

        @pl.when(t - lag == S - 2)
        def _():
            total(0, back, s)

        if relay:

            @pl.when(t < S)
            def _():
                for h in range(2):
                    bcopy(block(t), h).start()

        @pl.when(jnp.logical_and(t >= lag + 1, t - lag - 1 != S - 2))
        def _():
            zback(block(t - lag - 1)).start()

    def give_chunk(q):
        give(2 * q)
        give(2 * q + 1)

    pick(0)
    xg[0, s, :, cols(p)] = zs[0, s]
    xg[1, s, :, cols(p)] = zs[1, s]
    pick(1)
    xc[...] = jnp.zeros_like(xc)
    wait_entry()
    for i in range(2):
        spread(i, 0)

    def send_picked(k):
        @pl.when(k + 2 < S)
        def _():
            pick(k + 2)

        for i in range(2):
            zcopy(i, k + 1).start()

    loop(S - 1, send_picked)

    def hcopy(turn, k):
        to = lax.rem(s + (1 if k == 0 else S - 1), S)
        return remote(
            edge_ref.at[turn, 1 - k], halo_ref.at[turn, k],
            hsend.at[turn, k], hrecv.at[turn, k], sp=to,
        )

    sends = (s < S - 1, s > 0)
    takes = (s > 0, s < S - 1)

    def greet_edges(turn, value):
        edge_ref[turn, 0] = value[:8]
        edge_ref[turn, 1] = value[tokens - 8 :]

    def send_edges(turn):
        for k in range(2):

            @pl.when(sends[k])
            def _(k=k):
                hcopy(turn, k).start()

    def take_edges(turn, value):
        rim[8 : 8 + tokens] = value
        rim[0:8] = jnp.zeros_like(rim[0:8])
        rim[8 + tokens : 16 + tokens] = jnp.zeros_like(rim[0:8])
        for k in range(2):

            @pl.when(takes[k])
            def _(k=k):
                hcopy(turn, k).wait_recv()
                at = (0, 8 + tokens)[k]
                rim[at : at + 8] = halo_ref[turn, k]

    def mixed_in():
        return c_ref[...].astype(F32) * u_ref[...].astype(F32)

    for load in loads[4:6]:
        load.wait()
    greet_edges(0, mixed_in())

    def chunk(q):
        return pl.ds(pl.multiple_of(q * 2 * capp, 2 * capp), 2 * capp)

    def step(q):
        live, later, last = q < n, q > 0, q == n

        @pl.when(jnp.logical_and(live, later))
        def _():
            forward(0, 2 * q)

        @pl.when(later)
        def _():
            pass_on(1, 2 * q - 1)

        @pl.when(last)
        def _():
            give_chunk(n - 2)
            service(0)

        @pl.when(later)
        def _():
            ready(0, q - 1)

            @pl.when(q == 1)
            def _():
                for load in loads[6:9]:
                    load.wait()

            pre[...] = contract_last(xc[0, chunk(q - 1), :], gate_w[...])

        @pl.when(live)
        def _():
            forward(0, 2 * q + 1)
            pass_on(0, 2 * q)

        @pl.when(last)
        def _():
            service(1)

        @pl.when(later)
        def _():
            upre[...] = contract_last(xc[0, chunk(q - 1), :], up_w[...])

        @pl.when(jnp.logical_and(live, later))
        def _():
            forward(1, 2 * q)

        @pl.when(live)
        def _():
            pass_on(0, 2 * q + 1)

        @pl.when(last)
        def _():
            service(2)

        @pl.when(later)
        def _():
            ready(1, q - 1)
            grad_hidden = contract_last(xc[1, chunk(q - 1), :], down_w[...])
            gate_pre, up_pre = pre[...], upre[...]
            sigma = jax.nn.sigmoid(gate_pre)
            gate_act = gate_pre * sigma
            hid[chunk(q - 1), :] = (gate_act * up_pre).astype(BF16)
            gback[chunk(q - 1), :] = (
                grad_hidden * up_pre * sigma * (1.0 + gate_pre * (1.0 - sigma))
            ).astype(BF16)
            uback[chunk(q - 1), :] = (grad_hidden * gate_act).astype(BF16)

        @pl.when(live)
        def _():
            forward(1, 2 * q + 1)
            pass_on(1, 2 * q)

        @pl.when(last)
        def _():
            service(3)

        @pl.when(later)
        def _():
            def piece(f):
                value = jnp.dot(
                    gback[chunk(q - 1), :], gate_w[:, cols(f)], preferred_element_type=F32
                ) + jnp.dot(
                    uback[chunk(q - 1), :], up_w[:, cols(f)], preferred_element_type=F32
                )
                for b in range(2):
                    part[2 * (q - 1) + b, :, cols(f)] = value[
                        b * capp : b * capp + cap
                    ].astype(BF16)

            loop(T, piece)

        @pl.when(q == n - 1)
        def _():
            loop(n - 3, lambda k: give_chunk(k + 1))

        @pl.when(last)
        def _():
            give_chunk(n - 1)
            give_chunk(0)

    send_edges(0)
    loop(n + 1, step)

    for load in loads[9:]:
        load.wait()
    take_edges(0, mixed_in())
    taps = [taps_ref[i : i + 1, :] for i in range(3)]
    convolved = (
        taps[0] * rim[7 : 7 + tokens]
        + taps[1] * rim[8 : 8 + tokens]
        + taps[2] * rim[9 : 9 + tokens]
    )
    conv_ref[...] = convolved
    y_ref[...] = (b_ref[...].astype(F32) * convolved).astype(BF16)

    hid_t[...] = hid[...].T
    gback_t[...] = gback[...].T
    uback_t[...] = uback[...].T
    jobs = ((hid_t, 1, ddown_ref), (gback_t, 0, dgate_ref), (uback_t, 0, dup_ref))
    width = 512
    tiles = T * d // width

    def weight_piece(k):
        for which, (left, i, out) in enumerate(jobs):

            @pl.when(k // tiles == which)
            def _(left=left, i=i, out=out):
                at = pl.ds(pl.multiple_of(lax.rem(k, tiles) * width, width), width)
                out[:, at] = jnp.dot(
                    left[...], xc[i, :, at], preferred_element_type=F32
                ).astype(BF16)

    steps = S + lag + 1 - 4
    each = -(-3 * tiles // (steps - 1))

    def finish_step(t):
        for k in range(each):

            @pl.when(t * each + k < 3 * tiles)
            def _(k=k):
                weight_piece(t * each + k)

        service(t + 4)

    loop(steps, finish_step)

    total_ref[...] = gin_ref[...].astype(F32)

    def gathered(r):
        j = block(r)
        at = dest(j)

        @pl.when(j != 0)
        def _():
            zback(j, True).wait_recv()

        chosen = (slots == code_ref[pl.ds(at, 1), :]).astype(F32).astype(BF16)
        total_ref[...] += contract_first(chosen, back[at])

    loop(S, gathered)
    value = total_ref[...].astype(BF16)
    own_ref[...] = value
    full_ref[:, cols(p)] = value
    dy_ref[...] = jnp.zeros_like(dy_ref)
    width = proj.shape[1]

    if relay:

        def acopy(k, h, arriving=False):
            to = (xn, yn)[k]
            view = full_ref.at[:, halfcols(to if arriving else p, h)]
            return remote(view, view, asend.at[2 * k + h], arecv.at[2 * k + h], tp=to)

        def arelay(k, arriving=False):
            near, far = ((xn, yn), (yn, xn))[k]
            view = full_ref.at[:, halfcols(3 - p if arriving else near, k)]
            return remote(view, view, asend.at[4 + k], arecv.at[4 + k], tp=far)

        for h in range(2):
            acopy(0, h).start()
            acopy(1, 1 - h).start()

        def hand_on():
            for k in range(2):
                acopy(k, k, True).wait_recv()
                arelay(k).start()

        def near_piece(k):
            acopy(k, 1 - k, True).wait_recv()

        def far_piece():
            for k in range(2):
                arelay(k, True).wait_recv()

        order_in = (
            (p, hand_on),
            (xn, lambda: near_piece(0)),
            (yn, lambda: near_piece(1)),
            (3 - p, far_piece),
        )
        gathers = [acopy(k, h) for k in range(2) for h in range(2)] + [arelay(0), arelay(1)]
    else:

        def acopy(r, arriving=False):
            at = lax.rem(p - r + T, T) if arriving else p
            view = full_ref.at[:, cols(at)]
            return remote(
                view, view, asend.at[r - 1], arecv.at[r - 1], tp=lax.rem(p + r, T)
            )

        for r in range(1, T):
            acopy(r).start()
        order_in = ((p, lambda: None),) + tuple(
            (lax.rem(p - r + T, T), lambda r=r: acopy(r, True).wait_recv())
            for r in range(1, T)
        )
        gathers = [acopy(r) for r in range(1, T)]

    def gcopy(q):
        return remote(
            proj.at[2 * q + 1 - c], given.at[q], gsend.at[q], grecv.at[q], sp=s + 1 - 2 * c
        )

    def pcopy(q):
        return remote(pairs.at[q], arrived.at[z], psend.at[q], precv.at[z], sp=2 * q + c)

    def pcopy_in(q):
        return remote(pairs.at[q], arrived.at[q], psend.at[q], precv.at[q], sp=2 * q + c)

    def mix(q):
        piece = full_ref[:, cols(q)]
        dy_ref[...] += contract_last(piece, out_w[:, cols(q)])
        value = contract_first(piece, y_ref[...]).astype(BF16)
        proj[2 * q] = value[:width]
        proj[2 * q + 1] = value[width:]

    def pair(q):
        gcopy(q).wait_recv()
        both = proj[2 * q + c].astype(F32) + given[q].astype(F32)

        @pl.when(q == z)
        def _():
            sum_ref[...] = both

        @pl.when(q != z)
        def _():
            pairs[q] = both.astype(BF16)

    def post(q):
        @pl.when(q != z)
        def _():
            pcopy(q).start()

    for k, (q, arrive) in enumerate(order_in):
        if k == 0:
            mix(q)
            arrive()
            gcopy(q).start()
            continue
        arrive()
        mix(q)
        pair(order_in[k - 1][0])
        gcopy(q).start()
        post(order_in[k - 1][0])
    last_piece = order_in[-1][0]
    grad_mixed = dy_ref[...] * b_ref[...].astype(F32)
    greet_edges(1, grad_mixed)
    gb_ref[...] = (dy_ref[...] * conv_ref[...]).astype(BF16)
    pair(last_piece)
    send_edges(1)
    post(last_piece)
    take_edges(1, grad_mixed)
    grad_z = (
        taps[0] * rim[9 : 9 + tokens]
        + taps[1] * rim[8 : 8 + tokens]
        + taps[2] * rim[7 : 7 + tokens]
    )
    gc_ref[...] = (grad_z * u_ref[...].astype(F32)).astype(BF16)
    gu_ref[...] = (grad_z * c_ref[...].astype(F32)).astype(BF16)

    def collect(q):
        @pl.when(q != z)
        def _():
            pcopy_in(q).wait_recv()
            sum_ref[...] += arrived[q].astype(F32)
            pcopy(q).wait_send()

        gcopy(q).wait_send()

    def drain(j):
        for i in range(2):

            @pl.when(j > 0)
            def _(i=i):
                zcopy(i, j).wait_send()

            for k in range(len(partners)):
                fcopy(i, j, k).wait_send()
                if relay:
                    rcopy(i, j, k).wait_send()
        if relay:
            for h in range(2):
                tcopy(j, h, 0).wait_send()
                tcopy(j, h, 1).wait_send()
                bcopy(j, h).wait_send()
        else:
            for r in range(1, T):
                tcopy(j, r).wait_send()

    loop(S, drain)
    loop(S - 1, lambda k: zback(k + 1).wait_send())
    for gather in gathers:
        gather.wait_send()
    for turn in range(2):
        for k in range(2):

            @pl.when(sends[k])
            def _(turn=turn, k=k):
                hcopy(turn, k).wait_send()

    loop(n, collect)


def finish_kernel(count, *refs):
    sem = refs[2 * count]
    copies = [
        pltpu.make_async_copy(refs[i], refs[count + i], sem.at[i]) for i in range(count)
    ]
    for copy in copies:
        copy.start()
    for copy in copies:
        copy.wait()


def vmem(count):
    return [pl.BlockSpec(memory_space=pltpu.VMEM)] * count


def body(
    routes, route_weights, expert_inputs, out_grad, w_gate, w_up, w_down,
    conv_u, conv_b, conv_c, conv_taps, out_proj,
):
    S, T = lax.axis_size("sp"), lax.axis_size("tp")
    tokens, d = expert_inputs.shape
    channels = conv_u.shape[1]
    cap = 3 * tokens // S
    capp = padded_rows(cap)
    hidden = w_gate.shape[1]
    dma = pltpu.SemaphoreType.DMA
    ways = 2 if T == 4 else T - 1
    relays = (2, S, 2) if T == 4 else (1, 1, 1)
    if T == 4:
        pieces = 4
        shapes = ((2, 2, S, cap, d // 2), (2, S, cap, d // 2), (2, S, cap, d // 2))
    else:
        pieces = T - 1
        shapes = ((T - 1, S, cap, d), (8, 128), (8, 128))
    landing = [pltpu.VMEM(shape, BF16) for shape in shapes]
    width = T * d // S
    outs = (
        pltpu.VMEM((tokens, d), BF16),
        pltpu.VMEM((width, channels), F32),
        pltpu.VMEM((tokens, channels), BF16),
        pltpu.VMEM((tokens, channels), BF16),
        pltpu.VMEM((tokens, channels), BF16),
        pltpu.VMEM((hidden, T * d), BF16),
        pltpu.VMEM((hidden, T * d), BF16),
        pltpu.VMEM((hidden, T * d), BF16),
    )
    anywhere = pl.BlockSpec(memory_space=pl.ANY)
    results = pl.pallas_call(
        functools.partial(expert_kernel, S, T),
        out_shape=outs,
        in_specs=[anywhere] * 12,
        out_specs=tuple(vmem(8)),
        scratch_shapes=[
            pltpu.VMEM((2, tokens), jnp.int32),
            pltpu.VMEM((2, tokens), F32),
            pltpu.VMEM((tokens, d), BF16),
            pltpu.VMEM((tokens, d), BF16),
            pltpu.VMEM((hidden, T * d), BF16),
            pltpu.VMEM((hidden, T * d), BF16),
            pltpu.VMEM((hidden, T * d), BF16),
            pltpu.VMEM((tokens, channels), BF16),
            pltpu.VMEM((tokens, channels), BF16),
            pltpu.VMEM((tokens, channels), BF16),
            pltpu.VMEM((3, channels), F32),
            pltpu.VMEM((channels, T * d), BF16),
            pltpu.VMEM((S, tokens), jnp.int32),
            pltpu.VMEM((S, tokens), F32),
            pltpu.VMEM((2, S, cap, d), BF16),
            pltpu.VMEM((2, S, cap, T * d), BF16),
            pltpu.VMEM((2, S * capp, T * d), BF16),
            pltpu.VMEM((2 * capp, hidden), F32),
            pltpu.VMEM((2 * capp, hidden), F32),
            pltpu.VMEM((S * capp, hidden), BF16),
            pltpu.VMEM((S * capp, hidden), BF16),
            pltpu.VMEM((S * capp, hidden), BF16),
            pltpu.VMEM((hidden, S * capp), BF16),
            pltpu.VMEM((hidden, S * capp), BF16),
            pltpu.VMEM((hidden, S * capp), BF16),
            pltpu.VMEM((S, cap, T * d), BF16),
            *landing,
            pltpu.VMEM((S, cap, d), BF16),
            pltpu.VMEM((S, cap, d), BF16),
            pltpu.VMEM((tokens, d), F32),
            pltpu.VMEM((tokens, T * d), BF16),
            pltpu.VMEM((2, 2, 8, channels), F32),
            pltpu.VMEM((2, 2, 8, channels), F32),
            pltpu.VMEM((tokens + 16, channels), F32),
            pltpu.VMEM((tokens, channels), F32),
            pltpu.VMEM((tokens, channels), BF16),
            pltpu.VMEM((tokens, channels), F32),
            pltpu.VMEM((S, width, channels), BF16),
            pltpu.VMEM((S // 2, width, channels), BF16),
            pltpu.VMEM((S // 2, width, channels), BF16),
            pltpu.VMEM((S // 2, width, channels), BF16),
            dma((12,)),
            dma((2, S)),
            dma((2, S)),
            dma((2, S, ways)),
            dma((2, S, ways)),
            dma(relays),
            dma(relays),
            dma((S, pieces)),
            dma((S, pieces)),
            dma(relays[1:]),
            dma(relays[1:]),
            dma((S,)),
            dma((S,)),
            dma((6 if T == 4 else T - 1,)),
            dma((6 if T == 4 else T - 1,)),
            dma((2, 2)),
            dma((2, 2)),
            dma((S // 2,)),
            dma((S // 2,)),
            dma((S // 2,)),
            dma((S // 2,)),
        ],
        compiler_params=pltpu.CompilerParams(
            collective_id=0, has_side_effects=True, vmem_limit_bytes=46 * 2**20
        ),
        name="experts",
    )(
        routes.T, route_weights.T, expert_inputs, out_grad, w_gate, w_up, w_down,
        conv_u, conv_b, conv_c, conv_taps, out_proj,
    )
    grad_input, proj_sum, grad_u, grad_b, grad_c, grad_gate, grad_up, grad_down = pl.pallas_call(
        functools.partial(finish_kernel, 8),
        out_shape=tuple(jax.ShapeDtypeStruct(v.shape, v.dtype) for v in outs),
        in_specs=vmem(8),
        out_specs=(anywhere,) * 8,
        scratch_shapes=[dma((8,))],
        compiler_params=pltpu.CompilerParams(vmem_limit_bytes=8 * 2**20),
        name="finish",
    )(*[pltpu.with_memory_space_constraint(v, pltpu.VMEM) for v in results])
    return (
        grad_gate[None], grad_up[None], grad_down[None], grad_input, proj_sum,
        grad_u, grad_b, grad_c,
    )


def solution(mesh):
    in_specs = (
        P("sp", None),
        P("sp", None),
        P("sp", "tp"),
        P("sp", "tp"),
        P("sp", "tp", None),
        P("sp", "tp", None),
        P("sp", "tp", None),
        P("sp", "tp"),
        P("sp", "tp"),
        P("sp", "tp"),
        P(None, "tp"),
        P("tp", None),
    )
    out_specs = (
        P("sp", "tp", None),
        P("sp", "tp", None),
        P("sp", "tp", None),
        P("sp", "tp"),
        P("sp", "tp"),
        P("sp", "tp"),
        P("sp", "tp"),
        P("sp", "tp"),
    )
    return jax.shard_map(body, mesh=mesh, in_specs=in_specs, out_specs=out_specs, check_vma=False)
```

```python
import functools

import jax
import jax.numpy as jnp
from jax import lax
from jax.experimental import pallas as pl
from jax.experimental.pallas import tpu as pltpu
from jax.sharding import PartitionSpec as P

MESH = pl.DeviceIdType.MESH
F32 = jnp.float32
BF16 = jnp.bfloat16


def contract_first(left, right):
    return lax.dot_general(
        left, right, (((0,), (0,)), ((), ())), preferred_element_type=jnp.float32
    )


def contract_last(left, right):
    return lax.dot_general(
        left, right, (((1,), (1,)), ((), ())), preferred_element_type=jnp.float32
    )


def loop(count, step):
    lax.fori_loop(0, count, lambda i, c: (step(i), c)[1], 0)


def enter(sizes):
    barrier = pltpu.get_barrier_semaphore()
    for axis, size in sizes:
        me = lax.axis_index(axis)

        def greet(i, axis=axis, size=size, me=me):
            pl.semaphore_signal(
                barrier,
                inc=1,
                device_id={axis: lax.rem(me + i + 1, size)},
                device_id_type=MESH,
            )

        loop(size - 1, greet)
    return lambda: pl.semaphore_wait(barrier, sum(size - 1 for _, size in sizes))


def remote(src, dst, send, recv, **where):
    return pltpu.make_async_remote_copy(
        src_ref=src,
        dst_ref=dst,
        send_sem=send,
        recv_sem=recv,
        device_id=where,
        device_id_type=MESH,
    )


def slot_codes(routes, experts):
    count = routes.shape[1]
    names = lax.broadcasted_iota(jnp.int32, (experts, count), 0)
    first = (routes[0:1, :] == names).astype(F32)
    second = (routes[1:2, :] == names).astype(F32)
    early = lax.broadcasted_iota(jnp.int32, (count, count), 0)
    late = lax.broadcasted_iota(jnp.int32, (count, count), 1)
    before = (early < late).astype(F32).astype(BF16)
    rank = jnp.dot((first + second).astype(BF16), before, preferred_element_type=F32)
    code = jnp.where(first + second > 0.5, rank, -1.0).astype(jnp.int32)
    return code, first, second


def padded_rows(cap):
    return -(-cap // 16) * 16


def expert_kernel(
    S, T, routes_hbm, wts_hbm, xin_hbm, gin_hbm, gate_hbm, up_hbm, down_hbm,
    u_hbm, b_hbm, c_hbm, taps_hbm, outw_hbm,
    own_ref, sum_ref, gu_ref, gb_ref, gc_ref, dgate_ref, dup_ref, ddown_ref,
    routes_ref, wts_ref, xin_ref, gin_ref, gate_w, up_w, down_w,
    u_ref, b_ref, c_ref, taps_ref, out_w,
    code_ref, weight_ref, zs, xg, xc, pre, upre,
    hid, gback, uback, hid_t, gback_t, uback_t, part, landed, met, passed, summed, back, total_ref,
    full_ref, edge_ref, halo_ref, rim, conv_ref, y_ref, dy_ref, proj, given, pairs, arrived,
    isem, zsend, zrecv, fsend, frecv, rsend, rrecv,
    tsend, trecv, bsend, brecv, ysend, yrecv, asend, arecv, hsend, hrecv,
    gsend, grecv, psend, precv,
):
    s, p = lax.axis_index("sp"), lax.axis_index("tp")
    n = S // 2
    z, c = s // 2, lax.rem(s, 2)
    cap, d = summed.shape[1], summed.shape[2]
    tokens = own_ref.shape[0]
    capp = padded_rows(cap)
    half = d // 2
    relay = T == 4
    wait_entry = enter((("sp", S), ("tp", T)))

    loads = [
        pltpu.make_async_copy(src, dst, isem.at[i])
        for i, (src, dst) in enumerate(
            (
                (routes_hbm, routes_ref), (wts_hbm, wts_ref), (xin_hbm, xin_ref),
                (gin_hbm, gin_ref), (u_hbm, u_ref), (c_hbm, c_ref), (gate_hbm.at[0], gate_w),
                (up_hbm.at[0], up_w), (down_hbm.at[0], down_w), (b_hbm, b_ref),
                (taps_hbm, taps_ref), (outw_hbm, out_w),
            )
        )
    ]
    for load in loads:
        load.start()
    for load in loads[:4]:
        load.wait()

    def offset(q):
        odd = lax.rem(q, 2)
        return lax.rem(odd * ((q + 1) // 2) + (1 - odd) * (n - q // 2), n)

    def dest(j):
        return 2 * lax.rem(z + offset(j // 2), n) + lax.rem(c + j, 2)

    def origin(j):
        return 2 * lax.rem(z - offset(j // 2) + n, n) + lax.rem(c + j, 2)

    def cols(q):
        return pl.ds(pl.multiple_of(q * d, d), d)

    def halfcols(q, h):
        return pl.ds(pl.multiple_of(q * d + h * half, half), half)

    if relay:
        xn, yn = p + 1 - 2 * lax.rem(p, 2), lax.rem(p + 2, 4)
        partners = ((xn, xn), (yn, yn))
        order = ((xn, yn), (yn, xn))
    else:
        xn, yn = p, p
        partners = tuple(
            (lax.rem(p + r, T), lax.rem(p - r + T, T)) for r in range(1, T)
        )

    code, first, second = slot_codes(routes_ref[...], S)
    code_ref[...] = code
    weight_ref[...] = first * wts_ref[0:1, :] + second * wts_ref[1:2, :]
    slots = lax.broadcasted_iota(jnp.int32, (cap, code.shape[1]), 0)

    def pick(j):
        to = dest(j)
        mask = slots == code_ref[pl.ds(to, 1), :]
        chosen = mask.astype(F32).astype(BF16)
        zs[0, to] = jnp.dot(chosen, xin_ref[...], preferred_element_type=F32).astype(BF16)
        held = jnp.sum(
            jnp.where(mask, weight_ref[pl.ds(to, 1), :], 0.0), axis=1, keepdims=True
        )
        zs[1, to] = (held * jnp.dot(chosen, gin_ref[...], preferred_element_type=F32)).astype(BF16)

    def zcopy(i, j, arriving=False):
        to = dest(j)
        row = origin(j) if arriving else s
        return remote(
            zs.at[i, to], xg.at[i, row, :, cols(p)], zsend.at[i, j], zrecv.at[i, j], sp=to
        )

    def fcopy(i, j, k, arriving=False):
        to, whence = partners[k]
        view = xg.at[i, origin(j), :, cols(whence if arriving else p)]
        return remote(view, view, fsend.at[i, j, k], frecv.at[i, j, k], tp=to)

    def rcopy(i, j, k, arriving=False):
        near, far = ((xn, yn), (yn, xn))[k]
        view = xg.at[i, origin(j), :, halfcols(3 - p if arriving else near, k)]
        return remote(view, view, rsend.at[i, j, k], rrecv.at[i, j, k], tp=far)

    def spread(i, j):
        for k in range(len(partners)):
            fcopy(i, j, k).start()

    def forward(i, j):
        zcopy(i, j, True).wait_recv()
        spread(i, j)

    def pass_on(i, j):
        for k in range(len(partners)):
            fcopy(i, j, k, True).wait_recv()
            if relay:
                rcopy(i, j, k).start()

    def ready(i, q):
        for b in range(2):
            j = 2 * q + b
            if relay:
                for k in range(2):
                    rcopy(i, j, k, True).wait_recv()
            xc[i, pl.ds(pl.multiple_of(j * capp, capp), cap), :] = xg[i, origin(j)]

    def zback(j, arriving=False):
        row = dest(j) if arriving else s
        return remote(
            summed.at[j], back.at[row], ysend.at[j], yrecv.at[j], sp=origin(j)
        )

    if relay:

        def tcopy(j, h, k):
            to = order[h][0]
            return remote(
                part.at[j, :, halfcols(3 - p if k else to, h)],
                landed.at[h, k, j],
                tsend.at[j, 2 * h + k],
                trecv.at[j, 2 * h + k],
                tp=to,
            )

        def bcopy(j, h):
            return remote(
                passed.at[h, j], met.at[h, j], bsend.at[j, h], brecv.at[j, h], tp=order[h][1]
            )

        def give(j):
            for k in (1, 0):
                for h in range(2):
                    tcopy(j, h, k).start()

        def combine(j):
            for h in range(2):
                tcopy(j, h, 1).wait_recv()
                mine = part[j, :, halfcols(order[h][1], h)].astype(F32)
                passed[h, j] = (mine + landed[h, 1, j].astype(F32)).astype(BF16)

        def total(j, out, row):
            for h in range(2):
                tcopy(j, h, 0).wait_recv()
                bcopy(j, h).wait_recv()
                mine = part[j, :, halfcols(p, h)].astype(F32)
                mine = mine + landed[h, 0, j].astype(F32)
                mine = mine + met[h, j].astype(F32)
                out[row, :, h * half : (h + 1) * half] = mine.astype(BF16)

    else:

        def tcopy(j, r):
            q = lax.rem(p + r, T)
            return remote(
                part.at[j, :, cols(q)],
                landed.at[r - 1, j],
                tsend.at[j, r - 1],
                trecv.at[j, r - 1],
                tp=q,
            )

        def give(j):
            for r in range(1, T):
                tcopy(j, r).start()

        def total(j, out, row):
            for r in range(1, T):
                tcopy(j, r).wait_recv()
            value = part[j, :, cols(p)].astype(F32)
            for r in range(1, T):
                value = value + landed[r - 1, j].astype(F32)
            out[row] = value.astype(BF16)

    lag, behind = 3, 7

    def block(r):
        return lax.rem(r + 2, S)

    def gathered(r):
        j = block(r)
        at = dest(j)

        @pl.when(j != 0)
        def _():
            zback(j, True).wait_recv()

        chosen = (slots == code_ref[pl.ds(at, 1), :]).astype(F32).astype(BF16)
        total_ref[...] += contract_first(chosen, back[at])

    def service(t):
        if relay:

            @pl.when(t < S)
            def _():
                combine(block(t))

        @pl.when(jnp.logical_and(t >= lag, t < S + lag))
        def _():
            j = block(t - lag)

            @pl.when(j != 0)
            def _():
                total(j, summed, j)

            @pl.when(j == 0)
            def _():
                total(j, back, s)

        if relay:

            @pl.when(t < S)
            def _():
                for h in range(2):
                    bcopy(block(t), h).start()

        @pl.when(jnp.logical_and(t + 2 >= S - 2, t + 2 < S))
        def _():
            give(block(t + 2))

        @pl.when(jnp.logical_and(t > lag, t <= S + lag))
        def _():
            j = block(t - lag - 1)

            @pl.when(j != 0)
            def _():
                zback(j).start()

        @pl.when(jnp.logical_and(t >= behind, t < S + behind))
        def _():
            gathered(t - behind)

    def give_chunk(q):
        give(2 * q)
        give(2 * q + 1)

    pick(0)
    xg[0, s, :, cols(p)] = zs[0, s]
    xg[1, s, :, cols(p)] = zs[1, s]
    pick(1)
    xc[...] = jnp.zeros_like(xc)
    total_ref[...] = gin_ref[...].astype(F32)
    wait_entry()
    for i in range(2):
        spread(i, 0)

    def send_picked(k):
        @pl.when(k + 2 < S)
        def _():
            pick(k + 2)

        for i in range(2):
            zcopy(i, k + 1).start()

    loop(S - 1, send_picked)

    def hcopy(turn, k):
        to = lax.rem(s + (1 if k == 0 else S - 1), S)
        return remote(
            edge_ref.at[turn, 1 - k], halo_ref.at[turn, k],
            hsend.at[turn, k], hrecv.at[turn, k], sp=to,
        )

    sends = (s < S - 1, s > 0)
    takes = (s > 0, s < S - 1)

    def greet_edges(turn, value):
        edge_ref[turn, 0] = value[:8]
        edge_ref[turn, 1] = value[tokens - 8 :]

    def send_edges(turn):
        for k in range(2):

            @pl.when(sends[k])
            def _(k=k):
                hcopy(turn, k).start()

    def take_edges(turn, value):
        rim[8 : 8 + tokens] = value
        rim[0:8] = jnp.zeros_like(rim[0:8])
        rim[8 + tokens : 16 + tokens] = jnp.zeros_like(rim[0:8])
        for k in range(2):

            @pl.when(takes[k])
            def _(k=k):
                hcopy(turn, k).wait_recv()
                at = (0, 8 + tokens)[k]
                rim[at : at + 8] = halo_ref[turn, k]

    def mixed_in():
        return c_ref[...].astype(F32) * u_ref[...].astype(F32)

    for load in loads[4:6]:
        load.wait()
    greet_edges(0, mixed_in())

    def chunk(q):
        return pl.ds(pl.multiple_of(q * 2 * capp, 2 * capp), 2 * capp)

    early = 3

    def message(m):
        return lax.rem(m // 2, 2), 2 * (m // 4) + lax.rem(m, 2)

    def exchange(q, k):
        m = 4 * q + k

        @pl.when(m < 4 * n if k % 2 else jnp.logical_and(m > 3, m < 4 * n))
        def _():
            forward(*message(m))

        @pl.when(jnp.logical_and(m >= early, m < 4 * n + early))
        def _():
            pass_on(*message(m - early))

    def step(q):
        deep, last, over = q > 1, q == n, q == n + 1

        exchange(q, 0)

        @pl.when(deep)
        def _():
            upre[...] = contract_last(xc[0, chunk(q - 2), :], up_w[...])

        @pl.when(over)
        def _():
            service(1)

        exchange(q, 1)

        @pl.when(deep)
        def _():
            ready(1, q - 2)
            grad_hidden = contract_last(xc[1, chunk(q - 2), :], down_w[...])
            gate_pre, up_pre = pre[...], upre[...]
            sigma = jax.nn.sigmoid(gate_pre)
            gate_act = gate_pre * sigma
            hid[chunk(q - 2), :] = (gate_act * up_pre).astype(BF16)
            gback[chunk(q - 2), :] = (
                grad_hidden * up_pre * sigma * (1.0 + gate_pre * (1.0 - sigma))
            ).astype(BF16)
            uback[chunk(q - 2), :] = (grad_hidden * gate_act).astype(BF16)

        @pl.when(over)
        def _():
            service(2)

        exchange(q, 2)

        @pl.when(deep)
        def _():
            def piece(f):
                value = jnp.dot(
                    gback[chunk(q - 2), :], gate_w[:, cols(f)], preferred_element_type=F32
                ) + jnp.dot(
                    uback[chunk(q - 2), :], up_w[:, cols(f)], preferred_element_type=F32
                )
                for b in range(2):
                    part[2 * (q - 2) + b, :, cols(f)] = value[
                        b * capp : b * capp + cap
                    ].astype(BF16)

            loop(T, piece)

        @pl.when(last)
        def _():
            give_chunk(n - 2)

        @pl.when(over)
        def _():
            give_chunk(n - 1)
            service(3)

        exchange(q, 3)

        @pl.when(q == n - 1)
        def _():
            loop(n - 3, lambda k: give_chunk(k + 1))

        @pl.when(jnp.logical_and(q > 0, q <= n))
        def _():
            ready(0, q - 1)

            @pl.when(q == 1)
            def _():
                for load in loads[6:9]:
                    load.wait()

            pre[...] = contract_last(xc[0, chunk(q - 1), :], gate_w[...])

        @pl.when(last)
        def _():
            service(0)

    send_edges(0)
    loop(n + 2, step)

    for load in loads[9:]:
        load.wait()
    take_edges(0, mixed_in())
    taps = [taps_ref[i : i + 1, :] for i in range(3)]
    convolved = (
        taps[0] * rim[7 : 7 + tokens]
        + taps[1] * rim[8 : 8 + tokens]
        + taps[2] * rim[9 : 9 + tokens]
    )
    conv_ref[...] = convolved
    y_ref[...] = (b_ref[...].astype(F32) * convolved).astype(BF16)

    hid_t[...] = hid[...].T
    gback_t[...] = gback[...].T
    uback_t[...] = uback[...].T
    jobs = ((hid_t, 1, ddown_ref), (gback_t, 0, dgate_ref), (uback_t, 0, dup_ref))
    width = 512
    tiles = T * d // width

    def weight_piece(k):
        for which, (left, i, out) in enumerate(jobs):

            @pl.when(k // tiles == which)
            def _(left=left, i=i, out=out):
                at = pl.ds(pl.multiple_of(lax.rem(k, tiles) * width, width), width)
                out[:, at] = jnp.dot(
                    left[...], xc[i, :, at], preferred_element_type=F32
                ).astype(BF16)

    steps = S + behind - 4
    each = 2 if relay else -(-3 * tiles // steps)

    def finish_step(t):
        for k in range(each):

            @pl.when(t * each + k < 3 * tiles)
            def _(k=k):
                weight_piece(t * each + k)

        service(t + 4)

    loop(steps, finish_step)

    value = total_ref[...].astype(BF16)
    own_ref[...] = value
    full_ref[:, cols(p)] = value
    dy_ref[...] = jnp.zeros_like(dy_ref)
    width = proj.shape[1]

    if relay:

        def acopy(k, h, arriving=False):
            to = (xn, yn)[k]
            view = full_ref.at[:, halfcols(to if arriving else p, h)]
            return remote(view, view, asend.at[2 * k + h], arecv.at[2 * k + h], tp=to)

        def arelay(k, arriving=False):
            near, far = ((xn, yn), (yn, xn))[k]
            view = full_ref.at[:, halfcols(3 - p if arriving else near, k)]
            return remote(view, view, asend.at[4 + k], arecv.at[4 + k], tp=far)

        for h in range(2):
            acopy(0, h).start()
            acopy(1, 1 - h).start()

        def hand_on():
            for k in range(2):
                acopy(k, k, True).wait_recv()
                arelay(k).start()

        def near_piece(k):
            acopy(k, 1 - k, True).wait_recv()

        def far_piece():
            for k in range(2):
                arelay(k, True).wait_recv()

        order_in = (
            (p, hand_on),
            (xn, lambda: near_piece(0)),
            (yn, lambda: near_piece(1)),
            (3 - p, far_piece),
        )
        gathers = [acopy(k, h) for k in range(2) for h in range(2)] + [arelay(0), arelay(1)]
    else:

        def acopy(r, arriving=False):
            at = lax.rem(p - r + T, T) if arriving else p
            view = full_ref.at[:, cols(at)]
            return remote(
                view, view, asend.at[r - 1], arecv.at[r - 1], tp=lax.rem(p + r, T)
            )

        for r in range(1, T):
            acopy(r).start()
        order_in = ((p, lambda: None),) + tuple(
            (lax.rem(p - r + T, T), lambda r=r: acopy(r, True).wait_recv())
            for r in range(1, T)
        )
        gathers = [acopy(r) for r in range(1, T)]

    def gcopy(q):
        return remote(
            proj.at[2 * q + 1 - c], given.at[q], gsend.at[q], grecv.at[q], sp=s + 1 - 2 * c
        )

    def pcopy(q):
        return remote(pairs.at[q], arrived.at[z], psend.at[q], precv.at[z], sp=2 * q + c)

    def pcopy_in(q):
        return remote(pairs.at[q], arrived.at[q], psend.at[q], precv.at[q], sp=2 * q + c)

    def mix(q):
        piece = full_ref[:, cols(q)]
        dy_ref[...] += contract_last(piece, out_w[:, cols(q)])
        value = contract_first(piece, y_ref[...]).astype(BF16)
        proj[2 * q] = value[:width]
        proj[2 * q + 1] = value[width:]

    def pair(q):
        gcopy(q).wait_recv()
        both = proj[2 * q + c].astype(F32) + given[q].astype(F32)

        @pl.when(q == z)
        def _():
            sum_ref[...] = both

        @pl.when(q != z)
        def _():
            pairs[q] = both.astype(BF16)

    def post(q):
        @pl.when(q != z)
        def _():
            pcopy(q).start()

    for k, (q, arrive) in enumerate(order_in):
        if k == 0:
            mix(q)
            arrive()
            gcopy(q).start()
            continue
        arrive()
        mix(q)
        pair(order_in[k - 1][0])
        gcopy(q).start()
        post(order_in[k - 1][0])
    last_piece = order_in[-1][0]
    grad_mixed = dy_ref[...] * b_ref[...].astype(F32)
    greet_edges(1, grad_mixed)
    gb_ref[...] = (dy_ref[...] * conv_ref[...]).astype(BF16)
    pair(last_piece)
    send_edges(1)
    post(last_piece)
    take_edges(1, grad_mixed)
    grad_z = (
        taps[0] * rim[9 : 9 + tokens]
        + taps[1] * rim[8 : 8 + tokens]
        + taps[2] * rim[7 : 7 + tokens]
    )
    gc_ref[...] = (grad_z * u_ref[...].astype(F32)).astype(BF16)
    gu_ref[...] = (grad_z * c_ref[...].astype(F32)).astype(BF16)

    def collect(q):
        @pl.when(q != z)
        def _():
            pcopy_in(q).wait_recv()
            sum_ref[...] += arrived[q].astype(F32)
            pcopy(q).wait_send()

        gcopy(q).wait_send()

    def drain(j):
        for i in range(2):

            @pl.when(j > 0)
            def _(i=i):
                zcopy(i, j).wait_send()

            for k in range(len(partners)):
                fcopy(i, j, k).wait_send()
                if relay:
                    rcopy(i, j, k).wait_send()
        if relay:
            for h in range(2):
                tcopy(j, h, 0).wait_send()
                tcopy(j, h, 1).wait_send()
                bcopy(j, h).wait_send()
        else:
            for r in range(1, T):
                tcopy(j, r).wait_send()

    loop(S, drain)
    loop(S - 1, lambda k: zback(k + 1).wait_send())
    for gather in gathers:
        gather.wait_send()
    for turn in range(2):
        for k in range(2):

            @pl.when(sends[k])
            def _(turn=turn, k=k):
                hcopy(turn, k).wait_send()

    loop(n, collect)


def finish_kernel(count, *refs):
    sem = refs[2 * count]
    copies = [
        pltpu.make_async_copy(refs[i], refs[count + i], sem.at[i]) for i in range(count)
    ]
    for copy in copies:
        copy.start()
    for copy in copies:
        copy.wait()


def vmem(count):
    return [pl.BlockSpec(memory_space=pltpu.VMEM)] * count


def body(
    routes, route_weights, expert_inputs, out_grad, w_gate, w_up, w_down,
    conv_u, conv_b, conv_c, conv_taps, out_proj,
):
    S, T = lax.axis_size("sp"), lax.axis_size("tp")
    tokens, d = expert_inputs.shape
    channels = conv_u.shape[1]
    cap = 3 * tokens // S
    capp = padded_rows(cap)
    hidden = w_gate.shape[1]
    dma = pltpu.SemaphoreType.DMA
    ways = 2 if T == 4 else T - 1
    relays = (2, S, 2) if T == 4 else (1, 1, 1)
    if T == 4:
        pieces = 4
        shapes = ((2, 2, S, cap, d // 2), (2, S, cap, d // 2), (2, S, cap, d // 2))
    else:
        pieces = T - 1
        shapes = ((T - 1, S, cap, d), (8, 128), (8, 128))
    landing = [pltpu.VMEM(shape, BF16) for shape in shapes]
    width = T * d // S
    outs = (
        pltpu.VMEM((tokens, d), BF16),
        pltpu.VMEM((width, channels), F32),
        pltpu.VMEM((tokens, channels), BF16),
        pltpu.VMEM((tokens, channels), BF16),
        pltpu.VMEM((tokens, channels), BF16),
        pltpu.VMEM((hidden, T * d), BF16),
        pltpu.VMEM((hidden, T * d), BF16),
        pltpu.VMEM((hidden, T * d), BF16),
    )
    anywhere = pl.BlockSpec(memory_space=pl.ANY)
    results = pl.pallas_call(
        functools.partial(expert_kernel, S, T),
        out_shape=outs,
        in_specs=[anywhere] * 12,
        out_specs=tuple(vmem(8)),
        scratch_shapes=[
            pltpu.VMEM((2, tokens), jnp.int32),
            pltpu.VMEM((2, tokens), F32),
            pltpu.VMEM((tokens, d), BF16),
            pltpu.VMEM((tokens, d), BF16),
            pltpu.VMEM((hidden, T * d), BF16),
            pltpu.VMEM((hidden, T * d), BF16),
            pltpu.VMEM((hidden, T * d), BF16),
            pltpu.VMEM((tokens, channels), BF16),
            pltpu.VMEM((tokens, channels), BF16),
            pltpu.VMEM((tokens, channels), BF16),
            pltpu.VMEM((3, channels), F32),
            pltpu.VMEM((channels, T * d), BF16),
            pltpu.VMEM((S, tokens), jnp.int32),
            pltpu.VMEM((S, tokens), F32),
            pltpu.VMEM((2, S, cap, d), BF16),
            pltpu.VMEM((2, S, cap, T * d), BF16),
            pltpu.VMEM((2, S * capp, T * d), BF16),
            pltpu.VMEM((2 * capp, hidden), F32),
            pltpu.VMEM((2 * capp, hidden), F32),
            pltpu.VMEM((S * capp, hidden), BF16),
            pltpu.VMEM((S * capp, hidden), BF16),
            pltpu.VMEM((S * capp, hidden), BF16),
            pltpu.VMEM((hidden, S * capp), BF16),
            pltpu.VMEM((hidden, S * capp), BF16),
            pltpu.VMEM((hidden, S * capp), BF16),
            pltpu.VMEM((S, cap, T * d), BF16),
            *landing,
            pltpu.VMEM((S, cap, d), BF16),
            pltpu.VMEM((S, cap, d), BF16),
            pltpu.VMEM((tokens, d), F32),
            pltpu.VMEM((tokens, T * d), BF16),
            pltpu.VMEM((2, 2, 8, channels), F32),
            pltpu.VMEM((2, 2, 8, channels), F32),
            pltpu.VMEM((tokens + 16, channels), F32),
            pltpu.VMEM((tokens, channels), F32),
            pltpu.VMEM((tokens, channels), BF16),
            pltpu.VMEM((tokens, channels), F32),
            pltpu.VMEM((S, width, channels), BF16),
            pltpu.VMEM((S // 2, width, channels), BF16),
            pltpu.VMEM((S // 2, width, channels), BF16),
            pltpu.VMEM((S // 2, width, channels), BF16),
            dma((12,)),
            dma((2, S)),
            dma((2, S)),
            dma((2, S, ways)),
            dma((2, S, ways)),
            dma(relays),
            dma(relays),
            dma((S, pieces)),
            dma((S, pieces)),
            dma(relays[1:]),
            dma(relays[1:]),
            dma((S,)),
            dma((S,)),
            dma((6 if T == 4 else T - 1,)),
            dma((6 if T == 4 else T - 1,)),
            dma((2, 2)),
            dma((2, 2)),
            dma((S // 2,)),
            dma((S // 2,)),
            dma((S // 2,)),
            dma((S // 2,)),
        ],
        compiler_params=pltpu.CompilerParams(
            collective_id=0, has_side_effects=True, vmem_limit_bytes=46 * 2**20
        ),
        name="experts",
    )(
        routes.T, route_weights.T, expert_inputs, out_grad, w_gate, w_up, w_down,
        conv_u, conv_b, conv_c, conv_taps, out_proj,
    )
    grad_input, proj_sum, grad_u, grad_b, grad_c, grad_gate, grad_up, grad_down = pl.pallas_call(
        functools.partial(finish_kernel, 8),
        out_shape=tuple(jax.ShapeDtypeStruct(v.shape, v.dtype) for v in outs),
        in_specs=vmem(8),
        out_specs=(anywhere,) * 8,
        scratch_shapes=[dma((8,))],
        compiler_params=pltpu.CompilerParams(vmem_limit_bytes=8 * 2**20),
        name="finish",
    )(*[pltpu.with_memory_space_constraint(v, pltpu.VMEM) for v in results])
    return (
        grad_gate[None], grad_up[None], grad_down[None], grad_input, proj_sum,
        grad_u, grad_b, grad_c,
    )


def solution(mesh):
    in_specs = (
        P("sp", None),
        P("sp", None),
        P("sp", "tp"),
        P("sp", "tp"),
        P("sp", "tp", None),
        P("sp", "tp", None),
        P("sp", "tp", None),
        P("sp", "tp"),
        P("sp", "tp"),
        P("sp", "tp"),
        P(None, "tp"),
        P("tp", None),
    )
    out_specs = (
        P("sp", "tp", None),
        P("sp", "tp", None),
        P("sp", "tp", None),
        P("sp", "tp"),
        P("sp", "tp"),
        P("sp", "tp"),
        P("sp", "tp"),
        P("sp", "tp"),
    )
    return jax.shard_map(body, mesh=mesh, in_specs=in_specs, out_specs=out_specs, check_vma=False)
```

```python
import functools

import jax
import jax.numpy as jnp
from jax import lax
from jax.experimental import pallas as pl
from jax.experimental.pallas import tpu as pltpu
from jax.sharding import PartitionSpec as P

MESH = pl.DeviceIdType.MESH
F32 = jnp.float32
BF16 = jnp.bfloat16


def contract_first(left, right):
    return lax.dot_general(
        left, right, (((0,), (0,)), ((), ())), preferred_element_type=jnp.float32
    )


def contract_last(left, right):
    return lax.dot_general(
        left, right, (((1,), (1,)), ((), ())), preferred_element_type=jnp.float32
    )


def loop(count, step):
    lax.fori_loop(0, count, lambda i, c: (step(i), c)[1], 0)


def enter(sizes):
    barrier = pltpu.get_barrier_semaphore()
    for axis, size in sizes:
        me = lax.axis_index(axis)

        def greet(i, axis=axis, size=size, me=me):
            pl.semaphore_signal(
                barrier,
                inc=1,
                device_id={axis: lax.rem(me + i + 1, size)},
                device_id_type=MESH,
            )

        loop(size - 1, greet)
    return lambda: pl.semaphore_wait(barrier, sum(size - 1 for _, size in sizes))


def remote(src, dst, send, recv, **where):
    return pltpu.make_async_remote_copy(
        src_ref=src,
        dst_ref=dst,
        send_sem=send,
        recv_sem=recv,
        device_id=where,
        device_id_type=MESH,
    )


def slot_codes(routes, experts):
    count = routes.shape[1]
    names = lax.broadcasted_iota(jnp.int32, (experts, count), 0)
    first = (routes[0:1, :] == names).astype(F32)
    second = (routes[1:2, :] == names).astype(F32)
    early = lax.broadcasted_iota(jnp.int32, (count, count), 0)
    late = lax.broadcasted_iota(jnp.int32, (count, count), 1)
    before = (early < late).astype(F32).astype(BF16)
    rank = jnp.dot((first + second).astype(BF16), before, preferred_element_type=F32)
    code = jnp.where(first + second > 0.5, rank, -1.0).astype(jnp.int32)
    return code, first, second


def padded_rows(cap):
    return -(-cap // 16) * 16


def expert_kernel(
    S, T, routes_hbm, wts_hbm, xin_hbm, gin_hbm, gate_hbm, up_hbm, down_hbm,
    u_hbm, b_hbm, c_hbm, taps_hbm, outw_hbm,
    own_ref, sum_ref, gu_ref, gb_ref, gc_ref, dgate_ref, dup_ref, ddown_ref,
    routes_ref, wts_ref, xin_ref, gin_ref, gate_w, up_w, down_w,
    u_ref, b_ref, c_ref, taps_ref, out_w,
    code_ref, weight_ref, zs, xg, xc, pre, upre,
    hid, gback, uback, hid_t, gback_t, uback_t, part, landed, met, passed, summed, back, total_ref,
    full_ref, edge_ref, halo_ref, rim, conv_ref, y_ref, dy_ref, proj, given, pairs, arrived,
    isem, zsend, zrecv, fsend, frecv, rsend, rrecv,
    tsend, trecv, bsend, brecv, ysend, yrecv, asend, arecv, hsend, hrecv,
    gsend, grecv, psend, precv,
):
    s, p = lax.axis_index("sp"), lax.axis_index("tp")
    n = S // 2
    z, c = s // 2, lax.rem(s, 2)
    cap, d = summed.shape[1], summed.shape[2]
    tokens = own_ref.shape[0]
    capp = padded_rows(cap)
    half = d // 2
    relay = T == 4
    wait_entry = enter((("sp", S), ("tp", T)))

    loads = [
        pltpu.make_async_copy(src, dst, isem.at[i])
        for i, (src, dst) in enumerate(
            (
                (routes_hbm, routes_ref), (wts_hbm, wts_ref), (xin_hbm, xin_ref),
                (gin_hbm, gin_ref), (u_hbm, u_ref), (c_hbm, c_ref), (gate_hbm.at[0], gate_w),
                (up_hbm.at[0], up_w), (down_hbm.at[0], down_w), (b_hbm, b_ref),
                (taps_hbm, taps_ref), (outw_hbm, out_w),
            )
        )
    ]
    for load in loads:
        load.start()
    for load in loads[:4]:
        load.wait()

    def offset(q):
        odd = lax.rem(q, 2)
        return lax.rem(odd * ((q + 1) // 2) + (1 - odd) * (n - q // 2), n)

    def dest(j):
        return 2 * lax.rem(z + offset(j // 2), n) + lax.rem(c + j, 2)

    def origin(j):
        return 2 * lax.rem(z - offset(j // 2) + n, n) + lax.rem(c + j, 2)

    def cols(q):
        return pl.ds(pl.multiple_of(q * d, d), d)

    def halfcols(q, h):
        return pl.ds(pl.multiple_of(q * d + h * half, half), half)

    if relay:
        xn, yn = p + 1 - 2 * lax.rem(p, 2), lax.rem(p + 2, 4)
        partners = ((xn, xn), (yn, yn))
        order = ((xn, yn), (yn, xn))
    else:
        xn, yn = p, p
        partners = tuple(
            (lax.rem(p + r, T), lax.rem(p - r + T, T)) for r in range(1, T)
        )

    code, first, second = slot_codes(routes_ref[...], S)
    code_ref[...] = code
    weight_ref[...] = first * wts_ref[0:1, :] + second * wts_ref[1:2, :]
    slots = lax.broadcasted_iota(jnp.int32, (cap, code.shape[1]), 0)

    def pick(j):
        to = dest(j)
        mask = slots == code_ref[pl.ds(to, 1), :]
        chosen = mask.astype(F32).astype(BF16)
        zs[0, to] = jnp.dot(chosen, xin_ref[...], preferred_element_type=F32).astype(BF16)
        held = jnp.sum(
            jnp.where(mask, weight_ref[pl.ds(to, 1), :], 0.0), axis=1, keepdims=True
        )
        zs[1, to] = (held * jnp.dot(chosen, gin_ref[...], preferred_element_type=F32)).astype(BF16)

    def zcopy(i, j, arriving=False):
        to = dest(j)
        row = origin(j) if arriving else s
        return remote(
            zs.at[i, to], xg.at[i, row, :, cols(p)], zsend.at[i, j], zrecv.at[i, j], sp=to
        )

    def fcopy(i, j, k, arriving=False):
        to, whence = partners[k]
        view = xg.at[i, origin(j), :, cols(whence if arriving else p)]
        return remote(view, view, fsend.at[i, j, k], frecv.at[i, j, k], tp=to)

    def rcopy(i, j, k, arriving=False):
        near, far = ((xn, yn), (yn, xn))[k]
        view = xg.at[i, origin(j), :, halfcols(3 - p if arriving else near, k)]
        return remote(view, view, rsend.at[i, j, k], rrecv.at[i, j, k], tp=far)

    def spread(i, j):
        for k in range(len(partners)):
            fcopy(i, j, k).start()

    def forward(i, j):
        zcopy(i, j, True).wait_recv()
        spread(i, j)

    def pass_on(i, j):
        for k in range(len(partners)):
            fcopy(i, j, k, True).wait_recv()
            if relay:
                rcopy(i, j, k).start()

    def ready(i, q):
        for b in range(2):
            j = 2 * q + b
            if relay:
                for k in range(2):
                    rcopy(i, j, k, True).wait_recv()
            xc[i, pl.ds(pl.multiple_of(j * capp, capp), cap), :] = xg[i, origin(j)]

    def zback(j, arriving=False):
        row = dest(j) if arriving else s
        return remote(
            summed.at[j], back.at[row], ysend.at[j], yrecv.at[j], sp=origin(j)
        )

    if relay:

        def tcopy(j, h, k):
            to = order[h][0]
            return remote(
                part.at[j, :, halfcols(3 - p if k else to, h)],
                landed.at[h, k, j],
                tsend.at[j, 2 * h + k],
                trecv.at[j, 2 * h + k],
                tp=to,
            )

        def bcopy(j, h):
            return remote(
                passed.at[h, j], met.at[h, j], bsend.at[j, h], brecv.at[j, h], tp=order[h][1]
            )

        def give(j):
            for k in (1, 0):
                for h in range(2):
                    tcopy(j, h, k).start()

        def combine(j):
            for h in range(2):
                tcopy(j, h, 1).wait_recv()
                mine = part[j, :, halfcols(order[h][1], h)].astype(F32)
                passed[h, j] = (mine + landed[h, 1, j].astype(F32)).astype(BF16)

        def total(j, out, row):
            for h in range(2):
                tcopy(j, h, 0).wait_recv()
                bcopy(j, h).wait_recv()
                mine = part[j, :, halfcols(p, h)].astype(F32)
                mine = mine + landed[h, 0, j].astype(F32)
                mine = mine + met[h, j].astype(F32)
                out[row, :, h * half : (h + 1) * half] = mine.astype(BF16)

    else:

        def tcopy(j, r):
            q = lax.rem(p + r, T)
            return remote(
                part.at[j, :, cols(q)],
                landed.at[r - 1, j],
                tsend.at[j, r - 1],
                trecv.at[j, r - 1],
                tp=q,
            )

        def give(j):
            for r in range(1, T):
                tcopy(j, r).start()

        def total(j, out, row):
            for r in range(1, T):
                tcopy(j, r).wait_recv()
            value = part[j, :, cols(p)].astype(F32)
            for r in range(1, T):
                value = value + landed[r - 1, j].astype(F32)
            out[row] = value.astype(BF16)

    lag, behind = 2, 8

    def block(r):
        return lax.rem(r + 2, S)

    def gathered(r):
        j = block(r)
        at = dest(j)

        @pl.when(j != 0)
        def _():
            zback(j, True).wait_recv()

        chosen = (slots == code_ref[pl.ds(at, 1), :]).astype(F32).astype(BF16)
        total_ref[...] += contract_first(chosen, back[at])

    def service(t):
        if relay:

            @pl.when(t < S)
            def _():
                combine(block(t))

        @pl.when(jnp.logical_and(t >= lag, t < S + lag))
        def _():
            j = block(t - lag)

            @pl.when(j != 0)
            def _():
                total(j, summed, j)

            @pl.when(j == 0)
            def _():
                total(j, back, s)

        if relay:

            @pl.when(t < S)
            def _():
                for h in range(2):
                    bcopy(block(t), h).start()

        @pl.when(t == S - 4)
        def _():
            give_chunk(0)

        @pl.when(jnp.logical_and(t > lag, t <= S + lag))
        def _():
            j = block(t - lag - 1)

            @pl.when(j != 0)
            def _():
                zback(j).start()

        @pl.when(jnp.logical_and(t >= behind, t < S + behind))
        def _():
            gathered(t - behind)

    def give_chunk(q):
        if relay:
            for k in (1, 0):
                for b in range(2):
                    for h in range(2):
                        tcopy(2 * q + b, h, k).start()
        else:
            give(2 * q)
            give(2 * q + 1)

    pick(0)
    xg[0, s, :, cols(p)] = zs[0, s]
    xg[1, s, :, cols(p)] = zs[1, s]
    pick(1)
    xc[...] = jnp.zeros_like(xc)
    total_ref[...] = gin_ref[...].astype(F32)
    wait_entry()
    for i in range(2):
        spread(i, 0)

    def send_picked(k):
        @pl.when(k + 2 < S)
        def _():
            pick(k + 2)

        for i in range(2):
            zcopy(i, k + 1).start()

    loop(S - 1, send_picked)

    def hcopy(turn, k):
        to = lax.rem(s + (1 if k == 0 else S - 1), S)
        return remote(
            edge_ref.at[turn, 1 - k], halo_ref.at[turn, k],
            hsend.at[turn, k], hrecv.at[turn, k], sp=to,
        )

    sends = (s < S - 1, s > 0)
    takes = (s > 0, s < S - 1)

    def greet_edges(turn, value):
        edge_ref[turn, 0] = value[:8]
        edge_ref[turn, 1] = value[tokens - 8 :]

    def send_edges(turn):
        for k in range(2):

            @pl.when(sends[k])
            def _(k=k):
                hcopy(turn, k).start()

    def take_edges(turn, value):
        rim[8 : 8 + tokens] = value
        rim[0:8] = jnp.zeros_like(rim[0:8])
        rim[8 + tokens : 16 + tokens] = jnp.zeros_like(rim[0:8])
        for k in range(2):

            @pl.when(takes[k])
            def _(k=k):
                hcopy(turn, k).wait_recv()
                at = (0, 8 + tokens)[k]
                rim[at : at + 8] = halo_ref[turn, k]

    def mixed_in():
        return c_ref[...].astype(F32) * u_ref[...].astype(F32)

    for load in loads[4:6]:
        load.wait()
    greet_edges(0, mixed_in())

    def chunk(q):
        return pl.ds(pl.multiple_of(q * 2 * capp, 2 * capp), 2 * capp)

    early = 3

    def message(m):
        return lax.rem(m // 2, 2), 2 * (m // 4) + lax.rem(m, 2)

    def exchange(q, k):
        m = 4 * q + k

        @pl.when(m < 4 * n if k % 2 else jnp.logical_and(m > 3, m < 4 * n))
        def _():
            forward(*message(m))

        @pl.when(jnp.logical_and(m >= early, m < 4 * n + early))
        def _():
            pass_on(*message(m - early))

    def step(q):
        deep, last, over = q > 1, q == n, q == n + 1

        exchange(q, 0)

        @pl.when(deep)
        def _():
            upre[...] = contract_last(xc[0, chunk(q - 2), :], up_w[...])

        @pl.when(over)
        def _():
            service(1)

        exchange(q, 1)

        @pl.when(deep)
        def _():
            ready(1, q - 2)
            grad_hidden = contract_last(xc[1, chunk(q - 2), :], down_w[...])
            gate_pre, up_pre = pre[...], upre[...]
            sigma = jax.nn.sigmoid(gate_pre)
            gate_act = gate_pre * sigma
            hid[chunk(q - 2), :] = (gate_act * up_pre).astype(BF16)
            gback[chunk(q - 2), :] = (
                grad_hidden * up_pre * sigma * (1.0 + gate_pre * (1.0 - sigma))
            ).astype(BF16)
            uback[chunk(q - 2), :] = (grad_hidden * gate_act).astype(BF16)

        @pl.when(over)
        def _():
            service(2)

        exchange(q, 2)

        @pl.when(deep)
        def _():
            def piece(f):
                value = jnp.dot(
                    gback[chunk(q - 2), :], gate_w[:, cols(f)], preferred_element_type=F32
                ) + jnp.dot(
                    uback[chunk(q - 2), :], up_w[:, cols(f)], preferred_element_type=F32
                )
                for b in range(2):
                    part[2 * (q - 2) + b, :, cols(f)] = value[
                        b * capp : b * capp + cap
                    ].astype(BF16)

            loop(T, piece)

        @pl.when(last)
        def _():
            give_chunk(n - 2)

        @pl.when(over)
        def _():
            give_chunk(n - 1)
            service(3)

        exchange(q, 3)

        @pl.when(q == n - 1)
        def _():
            loop(n - 3, lambda k: give_chunk(k + 1))

        @pl.when(jnp.logical_and(q > 0, q <= n))
        def _():
            ready(0, q - 1)

            @pl.when(q == 1)
            def _():
                for load in loads[6:9]:
                    load.wait()

            pre[...] = contract_last(xc[0, chunk(q - 1), :], gate_w[...])

        @pl.when(last)
        def _():
            service(0)

    send_edges(0)
    loop(n + 2, step)

    for load in loads[9:]:
        load.wait()
    take_edges(0, mixed_in())
    taps = [taps_ref[i : i + 1, :] for i in range(3)]
    convolved = (
        taps[0] * rim[7 : 7 + tokens]
        + taps[1] * rim[8 : 8 + tokens]
        + taps[2] * rim[9 : 9 + tokens]
    )
    conv_ref[...] = convolved
    y_ref[...] = (b_ref[...].astype(F32) * convolved).astype(BF16)

    hid_t[...] = hid[...].T
    gback_t[...] = gback[...].T
    uback_t[...] = uback[...].T
    jobs = ((hid_t, 1, ddown_ref), (gback_t, 0, dgate_ref), (uback_t, 0, dup_ref))
    width = 512
    tiles = T * d // width

    def weight_piece(k):
        for which, (left, i, out) in enumerate(jobs):

            @pl.when(k // tiles == which)
            def _(left=left, i=i, out=out):
                at = pl.ds(pl.multiple_of(lax.rem(k, tiles) * width, width), width)
                out[:, at] = jnp.dot(
                    left[...], xc[i, :, at], preferred_element_type=F32
                ).astype(BF16)

    steps = S + behind - 4
    each = 2 if relay else -(-3 * tiles // steps)

    def finish_step(t):
        for k in range(each):

            @pl.when(t * each + k < 3 * tiles)
            def _(k=k):
                weight_piece(t * each + k)

        service(t + 4)

    loop(steps, finish_step)

    value = total_ref[...].astype(BF16)
    own_ref[...] = value
    full_ref[:, cols(p)] = value
    dy_ref[...] = jnp.zeros_like(dy_ref)
    width = proj.shape[1]

    if relay:

        def acopy(k, h, arriving=False):
            to = (xn, yn)[k]
            view = full_ref.at[:, halfcols(to if arriving else p, h)]
            return remote(view, view, asend.at[2 * k + h], arecv.at[2 * k + h], tp=to)

        def arelay(k, arriving=False):
            near, far = ((xn, yn), (yn, xn))[k]
            view = full_ref.at[:, halfcols(3 - p if arriving else near, k)]
            return remote(view, view, asend.at[4 + k], arecv.at[4 + k], tp=far)

        for h in range(2):
            acopy(0, h).start()
            acopy(1, 1 - h).start()

        def hand_on():
            for k in range(2):
                acopy(k, k, True).wait_recv()
                arelay(k).start()

        def near_piece(k):
            acopy(k, 1 - k, True).wait_recv()

        def far_piece():
            for k in range(2):
                arelay(k, True).wait_recv()

        order_in = (
            (p, hand_on),
            (xn, lambda: near_piece(0)),
            (yn, lambda: near_piece(1)),
            (3 - p, far_piece),
        )
        gathers = [acopy(k, h) for k in range(2) for h in range(2)] + [arelay(0), arelay(1)]
    else:

        def acopy(r, arriving=False):
            at = lax.rem(p - r + T, T) if arriving else p
            view = full_ref.at[:, cols(at)]
            return remote(
                view, view, asend.at[r - 1], arecv.at[r - 1], tp=lax.rem(p + r, T)
            )

        for r in range(1, T):
            acopy(r).start()
        order_in = ((p, lambda: None),) + tuple(
            (lax.rem(p - r + T, T), lambda r=r: acopy(r, True).wait_recv())
            for r in range(1, T)
        )
        gathers = [acopy(r) for r in range(1, T)]

    def gcopy(q):
        return remote(
            proj.at[2 * q + 1 - c], given.at[q], gsend.at[q], grecv.at[q], sp=s + 1 - 2 * c
        )

    def pcopy(q):
        return remote(pairs.at[q], arrived.at[z], psend.at[q], precv.at[z], sp=2 * q + c)

    def pcopy_in(q):
        return remote(pairs.at[q], arrived.at[q], psend.at[q], precv.at[q], sp=2 * q + c)

    def mix(q):
        piece = full_ref[:, cols(q)]
        dy_ref[...] += contract_last(piece, out_w[:, cols(q)])
        value = contract_first(piece, y_ref[...]).astype(BF16)
        proj[2 * q] = value[:width]
        proj[2 * q + 1] = value[width:]

    def pair(q):
        gcopy(q).wait_recv()
        both = proj[2 * q + c].astype(F32) + given[q].astype(F32)

        @pl.when(q == z)
        def _():
            sum_ref[...] = both

        @pl.when(q != z)
        def _():
            pairs[q] = both.astype(BF16)

    def post(q):
        @pl.when(q != z)
        def _():
            pcopy(q).start()

    for k, (q, arrive) in enumerate(order_in):
        if k == 0:
            mix(q)
            arrive()
            gcopy(q).start()
            continue
        arrive()
        mix(q)
        pair(order_in[k - 1][0])
        gcopy(q).start()
        post(order_in[k - 1][0])
    last_piece = order_in[-1][0]
    grad_mixed = dy_ref[...] * b_ref[...].astype(F32)
    greet_edges(1, grad_mixed)
    gb_ref[...] = (dy_ref[...] * conv_ref[...]).astype(BF16)
    pair(last_piece)
    send_edges(1)
    post(last_piece)
    take_edges(1, grad_mixed)
    grad_z = (
        taps[0] * rim[9 : 9 + tokens]
        + taps[1] * rim[8 : 8 + tokens]
        + taps[2] * rim[7 : 7 + tokens]
    )
    gc_ref[...] = (grad_z * u_ref[...].astype(F32)).astype(BF16)
    gu_ref[...] = (grad_z * c_ref[...].astype(F32)).astype(BF16)

    def collect(q):
        @pl.when(q != z)
        def _():
            pcopy_in(q).wait_recv()
            sum_ref[...] += arrived[q].astype(F32)
            pcopy(q).wait_send()

        gcopy(q).wait_send()

    def drain(j):
        for i in range(2):

            @pl.when(j > 0)
            def _(i=i):
                zcopy(i, j).wait_send()

            for k in range(len(partners)):
                fcopy(i, j, k).wait_send()
                if relay:
                    rcopy(i, j, k).wait_send()
        if relay:
            for h in range(2):
                tcopy(j, h, 0).wait_send()
                tcopy(j, h, 1).wait_send()
                bcopy(j, h).wait_send()
        else:
            for r in range(1, T):
                tcopy(j, r).wait_send()

    loop(S, drain)
    loop(S - 1, lambda k: zback(k + 1).wait_send())
    for gather in gathers:
        gather.wait_send()
    for turn in range(2):
        for k in range(2):

            @pl.when(sends[k])
            def _(turn=turn, k=k):
                hcopy(turn, k).wait_send()

    loop(n, collect)


def finish_kernel(count, *refs):
    sem = refs[2 * count]
    copies = [
        pltpu.make_async_copy(refs[i], refs[count + i], sem.at[i]) for i in range(count)
    ]
    for copy in copies:
        copy.start()
    for copy in copies:
        copy.wait()


def vmem(count):
    return [pl.BlockSpec(memory_space=pltpu.VMEM)] * count


def body(
    routes, route_weights, expert_inputs, out_grad, w_gate, w_up, w_down,
    conv_u, conv_b, conv_c, conv_taps, out_proj,
):
    S, T = lax.axis_size("sp"), lax.axis_size("tp")
    tokens, d = expert_inputs.shape
    channels = conv_u.shape[1]
    cap = 3 * tokens // S
    capp = padded_rows(cap)
    hidden = w_gate.shape[1]
    dma = pltpu.SemaphoreType.DMA
    ways = 2 if T == 4 else T - 1
    relays = (2, S, 2) if T == 4 else (1, 1, 1)
    if T == 4:
        pieces = 4
        shapes = ((2, 2, S, cap, d // 2), (2, S, cap, d // 2), (2, S, cap, d // 2))
    else:
        pieces = T - 1
        shapes = ((T - 1, S, cap, d), (8, 128), (8, 128))
    landing = [pltpu.VMEM(shape, BF16) for shape in shapes]
    width = T * d // S
    outs = (
        pltpu.VMEM((tokens, d), BF16),
        pltpu.VMEM((width, channels), F32),
        pltpu.VMEM((tokens, channels), BF16),
        pltpu.VMEM((tokens, channels), BF16),
        pltpu.VMEM((tokens, channels), BF16),
        pltpu.VMEM((hidden, T * d), BF16),
        pltpu.VMEM((hidden, T * d), BF16),
        pltpu.VMEM((hidden, T * d), BF16),
    )
    anywhere = pl.BlockSpec(memory_space=pl.ANY)
    results = pl.pallas_call(
        functools.partial(expert_kernel, S, T),
        out_shape=outs,
        in_specs=[anywhere] * 12,
        out_specs=tuple(vmem(8)),
        scratch_shapes=[
            pltpu.VMEM((2, tokens), jnp.int32),
            pltpu.VMEM((2, tokens), F32),
            pltpu.VMEM((tokens, d), BF16),
            pltpu.VMEM((tokens, d), BF16),
            pltpu.VMEM((hidden, T * d), BF16),
            pltpu.VMEM((hidden, T * d), BF16),
            pltpu.VMEM((hidden, T * d), BF16),
            pltpu.VMEM((tokens, channels), BF16),
            pltpu.VMEM((tokens, channels), BF16),
            pltpu.VMEM((tokens, channels), BF16),
            pltpu.VMEM((3, channels), F32),
            pltpu.VMEM((channels, T * d), BF16),
            pltpu.VMEM((S, tokens), jnp.int32),
            pltpu.VMEM((S, tokens), F32),
            pltpu.VMEM((2, S, cap, d), BF16),
            pltpu.VMEM((2, S, cap, T * d), BF16),
            pltpu.VMEM((2, S * capp, T * d), BF16),
            pltpu.VMEM((2 * capp, hidden), F32),
            pltpu.VMEM((2 * capp, hidden), F32),
            pltpu.VMEM((S * capp, hidden), BF16),
            pltpu.VMEM((S * capp, hidden), BF16),
            pltpu.VMEM((S * capp, hidden), BF16),
            pltpu.VMEM((hidden, S * capp), BF16),
            pltpu.VMEM((hidden, S * capp), BF16),
            pltpu.VMEM((hidden, S * capp), BF16),
            pltpu.VMEM((S, cap, T * d), BF16),
            *landing,
            pltpu.VMEM((S, cap, d), BF16),
            pltpu.VMEM((S, cap, d), BF16),
            pltpu.VMEM((tokens, d), F32),
            pltpu.VMEM((tokens, T * d), BF16),
            pltpu.VMEM((2, 2, 8, channels), F32),
            pltpu.VMEM((2, 2, 8, channels), F32),
            pltpu.VMEM((tokens + 16, channels), F32),
            pltpu.VMEM((tokens, channels), F32),
            pltpu.VMEM((tokens, channels), BF16),
            pltpu.VMEM((tokens, channels), F32),
            pltpu.VMEM((S, width, channels), BF16),
            pltpu.VMEM((S // 2, width, channels), BF16),
            pltpu.VMEM((S // 2, width, channels), BF16),
            pltpu.VMEM((S // 2, width, channels), BF16),
            dma((12,)),
            dma((2, S)),
            dma((2, S)),
            dma((2, S, ways)),
            dma((2, S, ways)),
            dma(relays),
            dma(relays),
            dma((S, pieces)),
            dma((S, pieces)),
            dma(relays[1:]),
            dma(relays[1:]),
            dma((S,)),
            dma((S,)),
            dma((6 if T == 4 else T - 1,)),
            dma((6 if T == 4 else T - 1,)),
            dma((2, 2)),
            dma((2, 2)),
            dma((S // 2,)),
            dma((S // 2,)),
            dma((S // 2,)),
            dma((S // 2,)),
        ],
        compiler_params=pltpu.CompilerParams(
            collective_id=0, has_side_effects=True, vmem_limit_bytes=46 * 2**20
        ),
        name="experts",
    )(
        routes.T, route_weights.T, expert_inputs, out_grad, w_gate, w_up, w_down,
        conv_u, conv_b, conv_c, conv_taps, out_proj,
    )
    grad_input, proj_sum, grad_u, grad_b, grad_c, grad_gate, grad_up, grad_down = pl.pallas_call(
        functools.partial(finish_kernel, 8),
        out_shape=tuple(jax.ShapeDtypeStruct(v.shape, v.dtype) for v in outs),
        in_specs=vmem(8),
        out_specs=(anywhere,) * 8,
        scratch_shapes=[dma((8,))],
        compiler_params=pltpu.CompilerParams(vmem_limit_bytes=8 * 2**20),
        name="finish",
    )(*[pltpu.with_memory_space_constraint(v, pltpu.VMEM) for v in results])
    return (
        grad_gate[None], grad_up[None], grad_down[None], grad_input, proj_sum,
        grad_u, grad_b, grad_c,
    )


def solution(mesh):
    in_specs = (
        P("sp", None),
        P("sp", None),
        P("sp", "tp"),
        P("sp", "tp"),
        P("sp", "tp", None),
        P("sp", "tp", None),
        P("sp", "tp", None),
        P("sp", "tp"),
        P("sp", "tp"),
        P("sp", "tp"),
        P(None, "tp"),
        P("tp", None),
    )
    out_specs = (
        P("sp", "tp", None),
        P("sp", "tp", None),
        P("sp", "tp", None),
        P("sp", "tp"),
        P("sp", "tp"),
        P("sp", "tp"),
        P("sp", "tp"),
        P("sp", "tp"),
    )
    return jax.shard_map(body, mesh=mesh, in_specs=in_specs, out_specs=out_specs, check_vma=False)
```
